32 devices in a mesh: sp: 16 (over z, y, core), tp: 2 (over x).
Axes of the slice: x: 2, y: 2, z: 4, core: 2. Of those that a mesh axis runs over, the one named last changes fastest.
Arguments:
- residual: bfloat16 [2048, 2048], P('sp', 'tp'), may hold values from -24 to 24
- queries: bfloat16 [2048, 2048], P('sp', 'tp'), may hold values from -16 to 16
- key_proj: bfloat16 [2048, 512], P(('sp', 'tp')), may hold values from -8 to 8
- value_proj: bfloat16 [2048, 512], P(('sp', 'tp')), may hold values from -6 to 6
- diff_lambda: float32 [8], replicated, may hold values from 0.3 to 0.8
- head_gain: float32 [256], replicated, may hold values from 0.1 to 1.9
- out_weight: bfloat16 [2048, 2048], P(None, 'tp'), may hold values from -0.125 to 0.125
- norm_gain: float32 [2048], P('tp'), may hold values from 0.1 to 1.9
- up_weight: bfloat16 [2048, 8192], P('sp', 'tp'), may hold values from -0.125 to 0.125
- down_weight: bfloat16 [8192, 2048], P('tp', 'sp'), may hold values from -0.0625 to 0.0625
Outputs:
- layer_out: bfloat16 [2048, 2048], P('sp', 'tp')
The draws below stay inside these ranges and needn't reach their ends.
All inputs are finite; a program needn't handle non-finite values.
Results may differ from the reference program's by a relative error of at most 0.012.
Values may be sent and summed in bfloat16 or wider, within the bound.
A program may use at most 128 MiB of HBM per device.

```python
import jax
import jax.numpy as jnp
from jax import lax

D = 2048
HEADS = 8
KV_HEADS = 2
HEAD_DIM = 128
VALUE_DIM = 256
FF = 8192
TOK_DEV = 128
SEQ = 2048


def draw_residual(key, part):
    base = jax.random.fold_in(key, 11)
    first, second, third = jax.random.split(base, 3)
    noise = jax.random.truncated_normal(first, -3.0, 3.0, (SEQ, D), jnp.float32)
    column = jnp.arange(D, dtype=jnp.float32) / D
    rough = jnp.exp(jax.random.uniform(second, (1, D), jnp.float32, jnp.log(0.8), jnp.log(1.25)))
    col_scale = jnp.exp(jnp.log(0.3) + jnp.log(10.0) * column)[None, :] * rough
    row_scale = jnp.exp(jax.random.uniform(third, (SEQ, 1), jnp.float32, jnp.log(0.5), jnp.log(1.6)))
    return (noise * col_scale * row_scale).astype(jnp.bfloat16)


def drawn_pair(key):
    base = jax.random.fold_in(key, 23)
    streams = jax.random.split(base, 2)
    query_vals = 1.3 * jax.random.truncated_normal(streams[0], -6.0, 6.0, (SEQ, HEADS * 2 * HEAD_DIM), jnp.float32)
    key_vals = 1.3 * jax.random.truncated_normal(streams[1], -6.0, 6.0, (SEQ, KV_HEADS * 2 * HEAD_DIM), jnp.float32)
    return (query_vals, key_vals)


def draw_queries(key, part):
    return drawn_pair(key)[0].astype(jnp.bfloat16)


def draw_key_proj(key, part):
    return drawn_pair(key)[1].astype(jnp.bfloat16)


def levels(own_key, extent, cuts, least, largest):
    def one(position, shards_of):
        heights = jax.random.uniform(jax.random.fold_in(jax.random.fold_in(own_key, 6), position), (shards_of,), jnp.float32, least / len(cuts), largest / len(cuts))
        return jnp.repeat(jnp.exp(heights), extent[position] // shards_of).reshape((-1,) + (1,) * (len(extent) - position - 1))

    loudness = one(*cuts[0])
    for cut in cuts[1:]:
        loudness = loudness * one(*cut)
    return loudness


def normal_values(own_key, shape, deviation, most, shards=(), held_as=jnp.bfloat16):
    values = jax.random.normal(own_key, shape, jnp.float32) * deviation
    if len(shards) > 0:
        values = levels(own_key, shape, shards, -0.22, 0.18) * values
    return jnp.clip(values, min=-most, max=most).astype(held_as)


def setup_inputs(seed: int = 0) -> dict:
    key_list = jax.random.split(jax.random.key(seed), 11)
    residual = draw_residual(jax.random.fold_in(key_list[10], 71), 0)
    queries = draw_queries(jax.random.fold_in(key_list[10], 71), 0)
    key_proj = draw_key_proj(jax.random.fold_in(key_list[10], 71), 0)
    value_proj = normal_values(key_list[3], (SEQ, KV_HEADS * VALUE_DIM), 1.0, 6.0, ((0, 32),))
    diff_lambda = jnp.clip(jax.random.uniform(key_list[4], (HEADS,), jnp.float32, 0.3, 0.8), 0.3, 0.8)
    head_gain = jnp.clip(1.0 + 0.18 * jax.random.normal(key_list[5], (VALUE_DIM,), jnp.float32), 0.1, 1.9)
    out_weight = normal_values(key_list[6], (HEADS * VALUE_DIM, D), (HEADS * VALUE_DIM) ** -0.5, 0.125, ((1, 2),))
    norm_gain = jnp.clip(1.0 + 0.18 * jax.random.normal(key_list[7], (D,), jnp.float32), 0.1, 1.9)
    up_weight = normal_values(key_list[8], (D, FF), D ** -0.5, 0.125, ((0, 16), (1, 2)))
    down_weight = normal_values(key_list[9], (FF, D), FF ** -0.5, 0.0625, ((0, 2), (1, 16)))
    return dict(residual=residual, queries=queries, key_proj=key_proj, value_proj=value_proj, diff_lambda=diff_lambda, head_gain=head_gain, out_weight=out_weight, norm_gain=norm_gain, up_weight=up_weight, down_weight=down_weight)


epsilon = 1e-06

def reference(residual, queries, key_proj, value_proj, diff_lambda, head_gain, out_weight, norm_gain, up_weight, down_weight):
    per_group = HEADS // KV_HEADS
    seq_len = queries.shape[0]
    scaling = HEAD_DIM ** (-0.5)
    key_grid = key_proj.astype(jnp.float32).reshape(seq_len, KV_HEADS, 2, HEAD_DIM)
    value_grid = value_proj.astype(jnp.float32).reshape(seq_len, KV_HEADS, VALUE_DIM)
    lambdas = diff_lambda.reshape(KV_HEADS, per_group, 1, 1)
    blocks = queries.reshape(seq_len // TOK_DEV, TOK_DEV, KV_HEADS, per_group, 2, HEAD_DIM)

    def one_block(query_block):
        query_float = query_block.astype(jnp.float32)
        scores = jnp.einsum('qagcd,kacd->agcqk', query_float, key_grid) * scaling
        highest = lax.optimization_barrier(jnp.max(scores, axis=-1, keepdims=True))
        weights = jnp.exp(scores - highest)
        totals = lax.optimization_barrier(jnp.sum(weights, axis=-1))
        rounded = lax.optimization_barrier(weights.astype(jnp.bfloat16)).astype(jnp.float32)
        summed = jnp.einsum('agcqk,kae->agcqe', rounded, value_grid)
        per_map = summed / totals[..., None]
        difference = per_map[:, :, 0] - lambdas * per_map[:, :, 1]
        normed = difference * lax.rsqrt(lax.optimization_barrier(jnp.mean(difference * difference, axis=-1, keepdims=True)) + epsilon) * head_gain
        return normed.astype(jnp.bfloat16).reshape(HEADS, TOK_DEV, VALUE_DIM)
    outputs = lax.map(one_block, blocks)
    head_outputs = outputs.transpose(1, 0, 2, 3).reshape(HEADS, seq_len, VALUE_DIM)
    out_grid = out_weight.reshape(HEADS, VALUE_DIM, D)
    projected = jnp.einsum('hse,hed->sd', head_outputs.astype(jnp.float32), out_grid.astype(jnp.float32))
    after_mix = residual.astype(jnp.float32) + projected
    normed = (after_mix * lax.rsqrt(lax.optimization_barrier(jnp.mean(after_mix * after_mix, axis=1, keepdims=True)) + epsilon) * norm_gain).astype(jnp.bfloat16)
    hidden = jnp.dot(normed, up_weight, preferred_element_type=jnp.float32)
    activated = jnp.square(jax.nn.relu(hidden)).astype(jnp.bfloat16)
    mixed = jnp.dot(activated, down_weight, preferred_element_type=jnp.float32)
    return (after_mix + mixed).astype(jnp.bfloat16)
```

```python
import functools
import math

import jax
import jax.numpy as jnp
from jax import lax
from jax.experimental import pallas as pl
from jax.experimental.pallas import tpu as pltpu
from jax.sharding import PartitionSpec as P

D = 2048
HEADS = 8
KV_HEADS = 2
HEAD_DIM = 128
VALUE_DIM = 256


epsilon = 1e-06


def head_norm(per_map, lambdas, gain):
    difference = per_map[:, 0] - lambdas[:, None, None] * per_map[:, 1]
    scaled = (
        difference
        * lax.rsqrt(jnp.mean(difference * difference, axis=-1, keepdims=True) + epsilon)
        * gain
    )
    return scaled.astype(jnp.bfloat16)


def on_device(
    residual,
    queries,
    key_proj,
    value_proj,
    diff_lambda,
    head_gain,
    out_weight,
    norm_gain,
    up_weight,
    down_weight,
):
    rows_here = residual.shape[0]
    per_group = HEADS // KV_HEADS
    scaling = HEAD_DIM ** (-0.5)
    all_queries = lax.all_gather(queries, "tp", axis=1, tiled=True)
    query_grid = all_queries.reshape(rows_here, KV_HEADS, per_group, 2, HEAD_DIM)
    stat_shape = (KV_HEADS, per_group, 2, rows_here)
    maxima = jnp.full(stat_shape, -1e30, jnp.float32)
    key_piece = lax.all_gather(key_proj, "sp", axis=0, tiled=True)
    value_piece = lax.all_gather(value_proj, "sp", axis=0, tiled=True)
    key_count = key_piece.shape[0]
    key_grid = key_piece.reshape(key_count, KV_HEADS, 2, HEAD_DIM)
    value_grid = value_piece.reshape(key_count, KV_HEADS, VALUE_DIM)
    scores = (
        jnp.einsum("qagcd,kacd->agcqk", query_grid, key_grid, preferred_element_type=jnp.float32)
        * scaling
    )
    highest = jnp.maximum(maxima, jnp.max(scores, axis=-1))
    weights = jnp.exp(scores - highest[..., None])
    totals = jnp.sum(weights, axis=-1)
    weighted = jnp.einsum(
        "agcqk,kae->agcqe",
        weights.astype(jnp.bfloat16),
        value_grid,
        preferred_element_type=jnp.float32,
    )
    maxima, totals, weighted = (highest, totals, weighted)
    maxima = maxima.reshape(HEADS, 2, rows_here)
    totals = totals.reshape(HEADS, 2, rows_here)
    weighted = weighted.reshape(HEADS, 2, rows_here, VALUE_DIM)
    tp_size = lax.axis_size("tp")
    local_heads = HEADS // tp_size
    got_max, got_tot, got_sum = (
        lax.all_to_all(maxima, "tp", split_axis=0, concat_axis=0, tiled=True),
        lax.all_to_all(totals, "tp", split_axis=0, concat_axis=0, tiled=True),
        lax.all_to_all(weighted, "tp", split_axis=0, concat_axis=0, tiled=True),
    )
    got_max = got_max.reshape(tp_size, local_heads, 2, rows_here)
    got_tot = got_tot.reshape(tp_size, local_heads, 2, rows_here)
    got_sum = got_sum.reshape(tp_size, local_heads, 2, rows_here, VALUE_DIM)
    highest = jnp.max(got_max, axis=0)
    factor = jnp.exp(got_max - highest)
    totals_all = jnp.sum(factor * got_tot, axis=0)
    sums_all = jnp.sum(factor[..., None] * got_sum, axis=0)
    lambdas = lax.dynamic_slice_in_dim(diff_lambda, lax.axis_index("tp") * local_heads, local_heads)
    own_heads = head_norm(sums_all / totals_all[..., None], lambdas, head_gain)
    head_outputs = lax.all_gather(own_heads, "tp", axis=0, tiled=True)
    out_grid = out_weight.reshape(HEADS, VALUE_DIM, out_weight.shape[1])
    projected = jnp.einsum(
        "hqe,hed->qd", head_outputs, out_grid, preferred_element_type=jnp.float32
    )
    after_mix = residual.astype(jnp.float32) + projected
    squares = lax.psum(jnp.sum(after_mix * after_mix, axis=1), "tp")
    normed = (after_mix * lax.rsqrt(squares / D + epsilon)[:, None] * norm_gain).astype(
        jnp.bfloat16
    )
    full_rows = lax.all_gather(normed, "tp", axis=1, tiled=True)
    hidden = jnp.dot(
        full_rows,
        lax.all_gather(up_weight, "sp", axis=0, tiled=True),
        preferred_element_type=jnp.float32,
    )
    activated = jnp.square(jax.nn.relu(hidden)).astype(jnp.bfloat16)
    partial_value = jnp.dot(
        activated,
        lax.all_gather(down_weight, "sp", axis=1, tiled=True),
        preferred_element_type=jnp.float32,
    )
    mixer_sum = lax.psum_scatter(partial_value, "tp", scatter_dimension=1, tiled=True)
    return (after_mix + mixer_sum).astype(jnp.bfloat16)


MESH = pl.DeviceIdType.MESH
F32 = jnp.float32
BF16 = jnp.bfloat16
CHIP_CORES = 2
Y_CHIPS = 2
Z_CHIPS = 4
OWN, NEAR, FIRST, SECOND = range(Z_CHIPS)


class Slots:
    def __init__(self):
        self.used = 0

    def take(self, count):
        base = self.used
        self.used += count
        return base


def fused_kernel(
    residual, queries, keys, values, lambdas, head_gain, out_weight, norm_gain,
    up, down, out,
    kv_all, up_all, down_all, q_buf, res_buf, w_buf, heads_all, squares, tokens, act,
    parts, parts_in, sum_out, sum_in, after, local_sem, send_sem, recv_sem,
):
    x = lax.axis_index("tp")
    s = lax.axis_index("sp")
    core, y, z = s % CHIP_CORES, (s // CHIP_CORES) % Y_CHIPS, s // (CHIP_CORES * Y_CHIPS)

    def place(z_, y_, c_):
        return (z_ * Y_CHIPS + y_) * CHIP_CORES + c_

    half = z // 2
    inner = ((z + 1) // 2) % 2
    z_near = 4 * half + 1 - z
    z_first = Z_CHIPS - 1 - z
    z_second = 5 - 4 * half - z_first
    z_in, z_out = 2 - half, 3 - 3 * half
    is_inner, is_outer = inner == 1, inner == 0

    def in_column(z_):
        return {"sp": place(z_, y, core), "tp": x}

    mate = {"sp": s, "tp": 1 - x}
    beside = {"sp": place(z, 1 - y, core), "tp": x}
    twin = {"sp": place(z, y, 1 - core), "tp": x}
    near, across, beyond = in_column(z_near), in_column(z_in), in_column(z_out)

    barrier = pltpu.get_barrier_semaphore()
    peers = [mate, beside, twin, near, across, beyond]
    for peer in peers:
        pl.semaphore_signal(barrier, inc=1, device_id=peer, device_id_type=MESH)

    count = {"local": 0, "remote": 0}
    slots = Slots()
    started = []

    def bring(src, dst):
        copy = pltpu.make_async_copy(src, dst, local_sem.at[count["local"]])
        count["local"] += 1
        copy.start()
        return copy

    def send(src, dst, peer, slot, when=None):
        i = count["remote"]
        count["remote"] += 1

        def copy():
            return pltpu.make_async_remote_copy(
                src_ref=src, dst_ref=dst, send_sem=send_sem.at[i], recv_sem=recv_sem.at[slot],
                device_id=peer, device_id_type=MESH,
            )

        if when is None:
            copy().start()
        else:
            pl.when(when)(lambda: copy().start())
        started.append((copy, when))

    def arrive(dst, slot):
        pltpu.make_async_remote_copy(
            src_ref=dst, dst_ref=dst, send_sem=send_sem.at[0], recv_sem=recv_sem.at[slot],
            device_id=mate, device_id_type=MESH,
        ).wait_recv()

    few = keys.shape[0]
    kw = kv_all.shape[2] // 2
    chunk = up_all.shape[2]
    lanes = down.shape[1]

    def half_of(ref, part):
        return ref.at[:, pl.ds(pl.multiple_of(part * kw, kw), kw)]

    def kv_rows(block, part, side):
        return kv_all.at[block, pl.ds(pl.multiple_of(part * few, few), few), pl.ds(side * kw, kw)]

    own_kv = [bring(half_of(keys, x), kv_rows(s, x, 0)), bring(half_of(values, x), kv_rows(s, x, 1))]
    q_copy = bring(queries, q_buf)

    pl.semaphore_wait(barrier, len(peers))

    swap = slots.take(2)
    for side, ref in enumerate((keys, values)):
        send(half_of(ref, 1 - x), kv_rows(s, x, side), mate, swap + side)
    w_copy = bring(out_weight, w_buf)
    r_copy = bring(residual, res_buf)

    def up_chunk(part):
        return up.at[:, pl.ds(pl.multiple_of(part * chunk, chunk), chunk)]

    def down_chunk(part):
        return down.at[pl.ds(pl.multiple_of(part * chunk, chunk), chunk), :]

    def kv_block(b):
        return kv_all.at[b]

    def up_block(b):
        return up_all.at[b]

    def down_block(b):
        return down_all.at[:, pl.ds(pl.multiple_of(b * lanes, lanes), lanes)]

    up_own = bring(up_chunk(z), up_block(s))
    down_own = bring(down_chunk(z), down_block(s))

    def multicast(block, base):
        send(block(z), block(z), near, base)
        send(block(z), block(z), across, base + 2 - inner)

    def relay(block, base, j):
        z_ = (z_in, z_out)[j]
        send(block(z_), block(z_), near, base + 1 + j, is_inner)

    class Stream:
        def __init__(self, block_of, order):
            self.block_of, self.order = block_of, order
            self.z, self.y, self.twin, self.far = (slots.take(Z_CHIPS) for _ in range(4))

        def block(self, k, y_, c_):
            return self.block_of(place(self.order[k], y_, c_))

        def wait_z(self, k):
            arrive(self.block(k, y, core), self.z + k)

        def spread(self, k):
            b = self.block(k, y, core)
            send(b, b, beside, self.y + k)
            send(b, b, twin, self.twin + k)

        def pass_on(self, k):
            b = self.block(k, 1 - y, core)
            arrive(b, self.y + k)
            send(b, b, twin, self.far + k)

        def wait_twin(self, k):
            arrive(self.block(k, y, 1 - core), self.twin + k)
            arrive(self.block(k, 1 - y, 1 - core), self.far + k)

    kv = Stream(kv_block, (z, z_near, z_in, z_out))
    ups = Stream(up_block, (z, z_near, z_first, z_second))
    downs = Stream(down_block, (z, z_near, z_first, z_second))

    def column_kv(z_):
        return kv_block(place(z_, y, core))

    for copy in own_kv:
        copy.wait()
    for side in range(2):
        arrive(kv_rows(s, 1 - x, side), swap + side)
    multicast(column_kv, kv.z + 1)
    kv.spread(OWN)
    for k in (NEAR, FIRST, SECOND):
        z_ = ups.order[k]
        send(up_chunk(z_), up_block(s), in_column(z_), ups.z + k)
    kv.wait_z(NEAR)
    kv.spread(NEAR)
    kv.pass_on(OWN)
    kv.wait_z(2)
    relay(column_kv, kv.z + 1, 0)
    kv.spread(2)
    kv.pass_on(NEAR)
    kv.wait_z(3)
    relay(column_kv, kv.z + 1, 1)
    kv.spread(3)
    up_own.wait()
    ups.spread(OWN)
    kv.pass_on(2)
    kv.pass_on(3)
    for k in range(Z_CHIPS):
        kv.wait_twin(k)
    q_copy.wait()

    local_heads = q_buf.shape[1] // (2 * HEAD_DIM)
    blocks, per_block = kv_all.shape[0], kv_all.shape[1]
    key_count = blocks * per_block
    factor = HEAD_DIM ** (-0.5) * math.log2(math.e)
    vals = lambda: kv_all[:, :, kw:].reshape(key_count, kw)
    heads = slots.take(local_heads)

    def head_cols(part, h):
        return heads_all.at[part, :, pl.ds(h * VALUE_DIM, VALUE_DIM)]

    for h in range(local_heads):
        maps = []
        for c in range(2):
            q = q_buf[:, (2 * h + c) * HEAD_DIM : (2 * h + c + 1) * HEAD_DIM]
            k = kv_all[:, :, c * HEAD_DIM : (c + 1) * HEAD_DIM].reshape(key_count, HEAD_DIM)
            scores = lax.dot_general(q, k, (((1,), (1,)), ((), ())), preferred_element_type=F32)
            top = jnp.max(scores, axis=1, keepdims=True)
            weights = jnp.exp2((scores - top) * factor)
            total = jnp.sum(weights, axis=1, keepdims=True)
            summed = jnp.dot(weights.astype(BF16), vals(), preferred_element_type=F32)
            maps.append(summed / total)
        diff = maps[0] - lambdas[x * local_heads + h] * maps[1]
        scaled = diff * lax.rsqrt(jnp.mean(diff * diff, axis=1, keepdims=True) + epsilon)
        heads_all[x, :, pl.ds(h * VALUE_DIM, VALUE_DIM)] = (scaled * head_gain[...]).astype(BF16)
        send(head_cols(x, h), head_cols(x, h), mate, heads + h)
        if h == 0:
            ups.wait_z(NEAR)
            ups.spread(NEAR)
        if h == 1:
            ups.pass_on(OWN)
        if h == local_heads - 1:
            ups.wait_z(FIRST)
            ups.spread(FIRST)

    wide = heads_all.shape[2]
    rows = heads_all.shape[1]
    w_copy.wait()
    r_copy.wait()

    def w_rows(part):
        return w_buf[pl.ds(pl.multiple_of(part * wide, wide), wide), :]

    mix = res_buf[...].astype(F32) + jnp.dot(heads_all[x], w_rows(x), preferred_element_type=F32)
    for h in range(local_heads):
        arrive(head_cols(1 - x, h), heads + h)
    mix = mix + jnp.dot(heads_all[1 - x], w_rows(1 - x), preferred_element_type=F32)
    after[...] = mix
    own_squares = jnp.sum(mix * mix, axis=1, keepdims=True)
    squares[x] = jnp.broadcast_to(own_squares, squares.shape[1:])
    square_slot = slots.take(1)
    send(squares.at[x], squares.at[x], mate, square_slot)
    arrive(squares.at[1 - x], square_slot)
    width = 2 * wide
    mean = (own_squares + squares[1 - x][:, :1]) / width
    tokens[z, x] = (after[...] * lax.rsqrt(mean + epsilon) * norm_gain[...]).astype(BF16)

    def column_tokens(z_):
        return tokens.at[z_, x]

    token_z = slots.take(Z_CHIPS - 1)
    token_x = slots.take(Z_CHIPS)

    def cross(z_, i):
        send(column_tokens(z_), column_tokens(z_), mate, token_x + i)

    def send_down(k):
        z_ = downs.order[k]
        send(down_chunk(z_), down_block(s), in_column(z_), downs.z + k)

    multicast(column_tokens, token_z)
    cross(z, OWN)
    send_down(FIRST)
    send_down(SECOND)
    ups.wait_z(SECOND)
    ups.spread(SECOND)
    ups.pass_on(NEAR)
    arrive(column_tokens(z_near), token_z)
    cross(z_near, NEAR)
    ups.pass_on(FIRST)
    for j, z_ in enumerate((z_in, z_out)):
        arrive(column_tokens(z_), token_z + 1 + j)
        relay(column_tokens, token_z, j)
        cross(z_, 2 + j)
    send_down(NEAR)
    down_own.wait()
    downs.spread(OWN)
    ups.pass_on(SECOND)
    for k in range(Z_CHIPS):
        ups.wait_twin(k)

    halves = up_all.shape[0] // 2

    def up_rows(i):
        return up_all[i * halves : (i + 1) * halves].reshape(wide, chunk)

    def activate(pair):
        first = pl.ds(2 * pair, 2)
        hidden = jnp.dot(
            tokens[first, 0].reshape(2 * rows, wide), up_rows(0), preferred_element_type=F32
        ) + jnp.dot(
            tokens[first, 1].reshape(2 * rows, wide), up_rows(1), preferred_element_type=F32
        )
        act[first] = jnp.square(jnp.maximum(hidden, 0.0)).astype(BF16).reshape(2, rows, chunk)

    for i, z_ in enumerate((z, z_near)):
        arrive(tokens.at[z_, 1 - x], token_x + i)
    activate(half)
    downs.pass_on(OWN)
    downs.wait_z(NEAR)
    downs.spread(NEAR)
    for i, z_ in ((2, z_in), (3, z_out)):
        arrive(tokens.at[z_, 1 - x], token_x + i)
    activate(1 - half)

    span = parts.shape[3]
    early_kept, early_sent = x == half, x != half
    part_slot = slots.take(2 * Z_CHIPS)
    to_visit = (z_in, z_out, z_near, z)

    def project(group):
        cols = down_all[:, pl.ds(pl.multiple_of(group * span, span), span)]
        product = jnp.dot(act[...].reshape(Z_CHIPS * rows, chunk), cols, preferred_element_type=F32)
        parts[group] = product.astype(BF16).reshape(Z_CHIPS, rows, span)

    def hand_over(group, when):
        a = group % 2
        for z_ in to_visit:
            send(parts.at[group, z_], parts_in.at[a, z_], mate,
                 part_slot + a * Z_CHIPS + z_, when)

    sum_slot = slots.take(4 * 2)

    def both(a, z_):
        arrive(parts_in.at[a, z_], part_slot + a * Z_CHIPS + z_)
        return parts[2 * x + a, z_].astype(F32) + parts_in[a, z_].astype(F32)

    def settle_own(a, when):
        @pl.when(when)
        def _():
            cols = pl.ds(pl.multiple_of(a * span, span), span)
            after[:, cols] = after[:, cols] + both(a, z)

    def deliver(a, i, row, peer, when):
        send(sum_out.at[i, a], sum_in.at[row, a], peer, sum_slot + 2 * row + a, when)

    def settle_near(a, when):
        @pl.when(when)
        def _():
            sum_out[0, a] = both(a, z_near).astype(BF16)

        deliver(a, 0, 0, near, when)

    def settle_far(a, j, when):
        z_ = (z_in, z_out)[j]

        @pl.when(when & is_outer)
        def _():
            sum_out[1 + j, a] = both(a, z_).astype(BF16)

        deliver(a, 1 + j, 2 + j, near, when & is_outer)

        @pl.when(when & is_inner)
        def _():
            mine = both(a, z_)
            arrive(sum_in.at[2 + j, a], sum_slot + 2 * (2 + j) + a)
            sum_out[1 + j, a] = (mine + sum_in[2 + j, a].astype(F32)).astype(BF16)

        deliver(a, 1 + j, 1, (across, beyond)[j], when & is_inner)

    for k in (OWN, NEAR):
        if k == NEAR:
            downs.pass_on(NEAR)
        downs.wait_twin(k)
    for i in range(2):
        project(2 * half + i)
        hand_over(2 * half + i, early_sent)

    downs.wait_z(FIRST)
    downs.spread(FIRST)
    downs.pass_on(FIRST)
    downs.wait_twin(FIRST)
    project(z_first)
    hand_over(z_first, early_kept)
    downs.wait_z(SECOND)
    downs.spread(SECOND)
    for j in range(2):
        settle_far(0, j, early_kept)
    settle_near(0, early_kept)
    settle_own(0, early_kept)
    downs.pass_on(SECOND)
    downs.wait_twin(SECOND)
    project(z_second)
    hand_over(z_second, early_kept)
    for j in range(2):
        settle_far(1, j, early_kept)
    settle_near(1, early_kept)
    settle_own(1, early_kept)

    late_outer, late_inner = early_sent & is_outer, early_sent & is_inner
    a_first, a_second = z_first % 2, z_second % 2
    for j in range(2):
        settle_far(a_first, j, late_outer)
    settle_near(a_first, early_sent)
    settle_own(a_first, early_sent)
    for j in range(2):
        settle_far(a_second, j, early_sent)
    settle_near(a_second, early_sent)
    settle_own(a_second, early_sent)
    for j in range(2):
        settle_far(a_first, j, late_inner)

    for row in range(2):
        for a in range(2):
            arrive(sum_in.at[row, a], sum_slot + 2 * row + a)
    for a in range(2):
        cols = slice(a * span, (a + 1) * span)
        total = after[:, cols] + sum_in[0, a].astype(F32) + sum_in[1, a].astype(F32)
        out[:, cols] = total.astype(out.dtype)
    for copy, when in started:
        if when is None:
            copy().wait_send()
        else:
            pl.when(when)(lambda: copy().wait_send())


def on_chip(sp_size, residual, queries, key_proj, value_proj, diff_lambda, head_gain, out_weight,
            norm_gain, up_weight, down_weight):
    rows, wide = residual.shape
    kw = key_proj.shape[1] // KV_HEADS
    chunk = up_weight.shape[1] // Z_CHIPS
    span = sp_size // Z_CHIPS * down_weight.shape[1]
    hbm = pl.BlockSpec(memory_space=pltpu.HBM)
    vmem = pl.BlockSpec(memory_space=pltpu.VMEM)
    smem = pl.BlockSpec(memory_space=pltpu.SMEM)
    copies = 160
    return pl.pallas_call(
        fused_kernel,
        out_shape=jax.ShapeDtypeStruct(residual.shape, BF16),
        in_specs=[hbm, hbm, hbm, hbm, smem, vmem, hbm, vmem, hbm, hbm],
        out_specs=vmem,
        scratch_shapes=[
            pltpu.VMEM((sp_size, 2 * key_proj.shape[0], 2 * kw), BF16),
            pltpu.VMEM((sp_size, up_weight.shape[0], chunk), BF16),
            pltpu.VMEM((chunk, sp_size * down_weight.shape[1]), BF16),
            pltpu.VMEM(queries.shape, BF16),
            pltpu.VMEM(residual.shape, BF16),
            pltpu.VMEM(out_weight.shape, BF16),
            pltpu.VMEM((2, rows, wide), BF16),
            pltpu.VMEM((2, rows, 128), F32),
            pltpu.VMEM((Z_CHIPS, 2, rows, wide), BF16),
            pltpu.VMEM((Z_CHIPS, rows, chunk), BF16),
            pltpu.VMEM((Z_CHIPS, Z_CHIPS, rows, span), BF16),
            pltpu.VMEM((2, Z_CHIPS, rows, span), BF16),
            pltpu.VMEM((3, 2, rows, span), BF16),
            pltpu.VMEM((4, 2, rows, span), BF16),
            pltpu.VMEM((rows, wide), F32),
            pltpu.SemaphoreType.DMA((8,)),
            pltpu.SemaphoreType.DMA((copies,)),
            pltpu.SemaphoreType.DMA((copies,)),
        ],
        compiler_params=pltpu.CompilerParams(
            collective_id=0, has_side_effects=True, vmem_limit_bytes=60 * 2**20
        ),
        name="fused_layer",
    )(residual, queries, key_proj, value_proj, diff_lambda, head_gain.reshape(1, -1), out_weight,
      norm_gain.reshape(1, -1), up_weight, down_weight)


def solution(mesh):
    sp_size, tp_size = mesh.shape["sp"], mesh.shape["tp"]
    direct = tp_size == KV_HEADS == 2 and sp_size == Z_CHIPS * Y_CHIPS * CHIP_CORES
    body = functools.partial(on_chip, sp_size) if direct else on_device
    return jax.shard_map(
        body,
        mesh=mesh,
        in_specs=(
            P("sp", "tp"),
            P("sp", "tp"),
            P(("sp", "tp"), None),
            P(("sp", "tp"), None),
            P(),
            P(),
            P(None, "tp"),
            P("tp"),
            P("sp", "tp"),
            P("tp", "sp"),
        ),
        out_specs=P("sp", "tp"),
        check_vma=False,
    )
```

```python
import functools
import math

import jax
import jax.numpy as jnp
from jax import lax
from jax.experimental import pallas as pl
from jax.experimental.pallas import tpu as pltpu
from jax.sharding import PartitionSpec as P

D = 2048
HEADS = 8
KV_HEADS = 2
HEAD_DIM = 128
VALUE_DIM = 256


epsilon = 1e-06


def head_norm(per_map, lambdas, gain):
    difference = per_map[:, 0] - lambdas[:, None, None] * per_map[:, 1]
    scaled = (
        difference
        * lax.rsqrt(jnp.mean(difference * difference, axis=-1, keepdims=True) + epsilon)
        * gain
    )
    return scaled.astype(jnp.bfloat16)


def on_device(
    residual,
    queries,
    key_proj,
    value_proj,
    diff_lambda,
    head_gain,
    out_weight,
    norm_gain,
    up_weight,
    down_weight,
):
    rows_here = residual.shape[0]
    per_group = HEADS // KV_HEADS
    scaling = HEAD_DIM ** (-0.5)
    all_queries = lax.all_gather(queries, "tp", axis=1, tiled=True)
    query_grid = all_queries.reshape(rows_here, KV_HEADS, per_group, 2, HEAD_DIM)
    stat_shape = (KV_HEADS, per_group, 2, rows_here)
    maxima = jnp.full(stat_shape, -1e30, jnp.float32)
    key_piece = lax.all_gather(key_proj, "sp", axis=0, tiled=True)
    value_piece = lax.all_gather(value_proj, "sp", axis=0, tiled=True)
    key_count = key_piece.shape[0]
    key_grid = key_piece.reshape(key_count, KV_HEADS, 2, HEAD_DIM)
    value_grid = value_piece.reshape(key_count, KV_HEADS, VALUE_DIM)
    scores = (
        jnp.einsum("qagcd,kacd->agcqk", query_grid, key_grid, preferred_element_type=jnp.float32)
        * scaling
    )
    highest = jnp.maximum(maxima, jnp.max(scores, axis=-1))
    weights = jnp.exp(scores - highest[..., None])
    totals = jnp.sum(weights, axis=-1)
    weighted = jnp.einsum(
        "agcqk,kae->agcqe",
        weights.astype(jnp.bfloat16),
        value_grid,
        preferred_element_type=jnp.float32,
    )
    maxima, totals, weighted = (highest, totals, weighted)
    maxima = maxima.reshape(HEADS, 2, rows_here)
    totals = totals.reshape(HEADS, 2, rows_here)
    weighted = weighted.reshape(HEADS, 2, rows_here, VALUE_DIM)
    tp_size = lax.axis_size("tp")
    local_heads = HEADS // tp_size
    got_max, got_tot, got_sum = (
        lax.all_to_all(maxima, "tp", split_axis=0, concat_axis=0, tiled=True),
        lax.all_to_all(totals, "tp", split_axis=0, concat_axis=0, tiled=True),
        lax.all_to_all(weighted, "tp", split_axis=0, concat_axis=0, tiled=True),
    )
    got_max = got_max.reshape(tp_size, local_heads, 2, rows_here)
    got_tot = got_tot.reshape(tp_size, local_heads, 2, rows_here)
    got_sum = got_sum.reshape(tp_size, local_heads, 2, rows_here, VALUE_DIM)
    highest = jnp.max(got_max, axis=0)
    factor = jnp.exp(got_max - highest)
    totals_all = jnp.sum(factor * got_tot, axis=0)
    sums_all = jnp.sum(factor[..., None] * got_sum, axis=0)
    lambdas = lax.dynamic_slice_in_dim(diff_lambda, lax.axis_index("tp") * local_heads, local_heads)
    own_heads = head_norm(sums_all / totals_all[..., None], lambdas, head_gain)
    head_outputs = lax.all_gather(own_heads, "tp", axis=0, tiled=True)
    out_grid = out_weight.reshape(HEADS, VALUE_DIM, out_weight.shape[1])
    projected = jnp.einsum(
        "hqe,hed->qd", head_outputs, out_grid, preferred_element_type=jnp.float32
    )
    after_mix = residual.astype(jnp.float32) + projected
    squares = lax.psum(jnp.sum(after_mix * after_mix, axis=1), "tp")
    normed = (after_mix * lax.rsqrt(squares / D + epsilon)[:, None] * norm_gain).astype(
        jnp.bfloat16
    )
    full_rows = lax.all_gather(normed, "tp", axis=1, tiled=True)
    hidden = jnp.dot(
        full_rows,
        lax.all_gather(up_weight, "sp", axis=0, tiled=True),
        preferred_element_type=jnp.float32,
    )
    activated = jnp.square(jax.nn.relu(hidden)).astype(jnp.bfloat16)
    partial_value = jnp.dot(
        activated,
        lax.all_gather(down_weight, "sp", axis=1, tiled=True),
        preferred_element_type=jnp.float32,
    )
    mixer_sum = lax.psum_scatter(partial_value, "tp", scatter_dimension=1, tiled=True)
    return (after_mix + mixer_sum).astype(jnp.bfloat16)


MESH = pl.DeviceIdType.MESH
F32 = jnp.float32
BF16 = jnp.bfloat16
CHIP_CORES = 2
Y_CHIPS = 2
Z_CHIPS = 4
OWN, NEAR, FAR, MID = range(Z_CHIPS)


class Slots:
    def __init__(self):
        self.used = 0

    def take(self, count):
        base = self.used
        self.used += count
        return base


def fused_kernel(
    residual, queries, keys, values, lambdas, head_gain, out_weight, norm_gain,
    up, down, out,
    kv_all, up_all, down_all, q_buf, res_buf, w_buf, heads_all, squares, tokens, act,
    parts, parts_in, sum_out, sum_in, after, local_sem, send_sem, recv_sem,
):
    x = lax.axis_index("tp")
    s = lax.axis_index("sp")
    core, y, z = s % CHIP_CORES, (s // CHIP_CORES) % Y_CHIPS, s // (CHIP_CORES * Y_CHIPS)

    def place(z_, y_, c_):
        return (z_ * Y_CHIPS + y_) * CHIP_CORES + c_

    half = z // 2
    inner = ((z + 1) // 2) % 2
    z_near = 4 * half + 1 - z
    z_in, z_out = 2 - half, 3 - 3 * half
    is_inner, is_outer = inner == 1, inner == 0

    def in_column(z_):
        return {"sp": place(z_, y, core), "tp": x}

    mate = {"sp": s, "tp": 1 - x}
    beside = {"sp": place(z, 1 - y, core), "tp": x}
    twin = {"sp": place(z, y, 1 - core), "tp": x}
    near, across, beyond = in_column(z_near), in_column(z_in), in_column(z_out)

    barrier = pltpu.get_barrier_semaphore()
    peers = [mate, beside, twin, near, across, beyond]
    for peer in peers:
        pl.semaphore_signal(barrier, inc=1, device_id=peer, device_id_type=MESH)

    count = {"local": 0, "remote": 0}
    slots = Slots()
    started = []

    def bring(src, dst):
        copy = pltpu.make_async_copy(src, dst, local_sem.at[count["local"]])
        count["local"] += 1
        copy.start()
        return copy

    def send(src, dst, peer, slot, when=None, waits=True):
        i = count["remote"]
        count["remote"] += 1

        def copy():
            return pltpu.make_async_remote_copy(
                src_ref=src, dst_ref=dst, send_sem=send_sem.at[i], recv_sem=recv_sem.at[slot],
                device_id=peer, device_id_type=MESH,
            )

        if when is None:
            copy().start()
        else:
            pl.when(when)(lambda: copy().start())
        if waits:
            started.append((copy, when))
        return copy

    def arrive(dst, slot, when=None):
        if when is not None:
            pl.when(when)(lambda: arrive(dst, slot))
            return
        pltpu.make_async_remote_copy(
            src_ref=dst, dst_ref=dst, send_sem=send_sem.at[0], recv_sem=recv_sem.at[slot],
            device_id=mate, device_id_type=MESH,
        ).wait_recv()

    few = keys.shape[0]
    kw = kv_all.shape[2] // 2
    chunk = up_all.shape[2]
    lanes = down.shape[1]

    def half_of(ref, part):
        return ref.at[:, pl.ds(pl.multiple_of(part * kw, kw), kw)]

    def kv_rows(block, part, side):
        return kv_all.at[block, pl.ds(pl.multiple_of(part * few, few), few), pl.ds(side * kw, kw)]

    own_kv = [bring(half_of(keys, x), kv_rows(s, x, 0)), bring(half_of(values, x), kv_rows(s, x, 1))]
    q_copy = bring(queries, q_buf)

    pl.semaphore_wait(barrier, len(peers))

    swap = slots.take(2)
    for side, ref in enumerate((keys, values)):
        send(half_of(ref, 1 - x), kv_rows(s, x, side), mate, swap + side)
    w_copy = bring(out_weight, w_buf)
    r_copy = bring(residual, res_buf)

    def up_chunk(part):
        return up.at[:, pl.ds(pl.multiple_of(part * chunk, chunk), chunk)]

    def down_chunk(part):
        return down.at[pl.ds(pl.multiple_of(part * chunk, chunk), chunk), :]

    def kv_block(b):
        return kv_all.at[b]

    def up_block(b):
        return up_all.at[b]

    def down_block(b):
        return down_all.at[:, pl.ds(pl.multiple_of(b * lanes, lanes), lanes)]

    up_own = bring(up_chunk(z), up_block(s))
    down_own = bring(down_chunk(z), down_block(s))

    def multicast(block, base):
        send(block(z), block(z), near, base)
        send(block(z), block(z), across, base + 2 - inner)

    def relay(block, base, j):
        z_ = (z_in, z_out)[j]
        send(block(z_), block(z_), near, base + 1 + j, is_inner)

    class Stream:
        def __init__(self, block_of, order):
            self.block_of, self.order = block_of, order
            self.z, self.y, self.twin, self.far = (slots.take(Z_CHIPS) for _ in range(4))

        def block(self, k, y_, c_):
            return self.block_of(place(self.order[k], y_, c_))

        def spread(self, k, when=None):
            b = self.block(k, y, core)
            if k != OWN:
                arrive(b, self.z + k, when)
            send(b, b, beside, self.y + k, when)
            send(b, b, twin, self.twin + k, when)

        def pass_on(self, k):
            b = self.block(k, 1 - y, core)
            arrive(b, self.y + k)
            send(b, b, twin, self.far + k)

        def wait_twin(self, k):
            arrive(self.block(k, y, 1 - core), self.twin + k)
            arrive(self.block(k, 1 - y, 1 - core), self.far + k)

    kv = Stream(kv_block, (z, z_near, z_in, z_out))
    ups = Stream(up_block, (z, z_near, z_out, z_in))
    downs = Stream(down_block, (z, z_near, z_out, z_in))

    def deal(stream, piece_of, k, when=None):
        z_, peer, slot = {
            NEAR: (z_near, near, NEAR), FAR: (z_out, beyond, FAR + inner), MID: (z_in, across, FAR + inner),
        }[k]
        send(piece_of(z_), stream.block_of(s), peer, stream.z + slot, when)

    def kv_onward(k):
        b = kv.block(k, y, core)
        send(b, b, beside, kv.y + k)
        send(b, b, twin, kv.twin + k)

    def column_kv(z_):
        return kv_block(place(z_, y, core))

    outlets = (
        (beside, kv.y), (twin, kv.twin), (near, kv.z + 1), (across, kv.z + 3 - inner)
    )
    for peer, slot in outlets:
        for side, ref in enumerate((keys, values)):
            send(half_of(ref, x), kv_rows(s, x, side), peer, slot)
    for side in range(2):
        arrive(kv_rows(s, 1 - x, side), swap + side)
    mates_rows = kv_all.at[s, pl.ds(pl.multiple_of((1 - x) * few, few), few), :]
    for peer, slot in outlets:
        send(mates_rows, mates_rows, peer, slot)
    deal(ups, up_chunk, NEAR, is_outer)
    deal(ups, up_chunk, MID)
    kv.spread(1)
    arrive(kv.block(2, y, core), kv.z + 2)
    relay(column_kv, kv.z + 1, 0)
    arrive(kv.block(3, y, core), kv.z + 3, is_inner)
    relay(column_kv, kv.z + 1, 1)
    deal(ups, up_chunk, NEAR, is_inner)
    kv_onward(2)
    arrive(kv.block(3, y, core), kv.z + 3, is_outer)
    deal(ups, up_chunk, FAR)
    kv_onward(3)
    up_own.wait()
    ups.spread(OWN)
    for copy in own_kv:
        copy.wait()
    for k in range(Z_CHIPS):
        kv.pass_on(k)
    for k in range(Z_CHIPS):
        kv.wait_twin(k)
    q_copy.wait()

    local_heads = q_buf.shape[1] // (2 * HEAD_DIM)
    blocks, per_block = kv_all.shape[0], kv_all.shape[1]
    key_count = blocks * per_block
    factor = HEAD_DIM ** (-0.5) * math.log2(math.e)
    vals = lambda: kv_all[:, :, kw:].reshape(key_count, kw)
    heads = slots.take(local_heads)

    def head_cols(part, h):
        return heads_all.at[part, :, pl.ds(h * VALUE_DIM, VALUE_DIM)]

    for h in range(local_heads):
        maps = []
        for c in range(2):
            q = q_buf[:, (2 * h + c) * HEAD_DIM : (2 * h + c + 1) * HEAD_DIM]
            k = kv_all[:, :, c * HEAD_DIM : (c + 1) * HEAD_DIM].reshape(key_count, HEAD_DIM)
            scores = lax.dot_general(q, k, (((1,), (1,)), ((), ())), preferred_element_type=F32)
            top = jnp.max(scores, axis=1, keepdims=True)
            weights = jnp.exp2((scores - top) * factor)
            total = jnp.sum(weights, axis=1, keepdims=True)
            summed = jnp.dot(weights.astype(BF16), vals(), preferred_element_type=F32)
            maps.append(summed / total)
        diff = maps[0] - lambdas[x * local_heads + h] * maps[1]
        scaled = diff * lax.rsqrt(jnp.mean(diff * diff, axis=1, keepdims=True) + epsilon)
        heads_all[x, :, pl.ds(h * VALUE_DIM, VALUE_DIM)] = (scaled * head_gain[...]).astype(BF16)
        send(head_cols(x, h), head_cols(x, h), mate, heads + h)
        if h < 2:
            ups.spread((NEAR, FAR)[h], is_inner)
    ups.spread(MID, is_inner)
    ups.spread(NEAR, is_outer)
    ups.pass_on(OWN)

    wide = heads_all.shape[2]
    rows = heads_all.shape[1]
    w_copy.wait()
    r_copy.wait()

    def w_rows(part):
        return w_buf[pl.ds(pl.multiple_of(part * wide, wide), wide), :]

    mix = res_buf[...].astype(F32) + jnp.dot(heads_all[x], w_rows(x), preferred_element_type=F32)
    for h in range(local_heads):
        arrive(head_cols(1 - x, h), heads + h)
    mix = mix + jnp.dot(heads_all[1 - x], w_rows(1 - x), preferred_element_type=F32)
    after[...] = mix
    own_squares = jnp.sum(mix * mix, axis=1, keepdims=True)
    squares[x] = jnp.broadcast_to(own_squares, squares.shape[1:])
    square_slot = slots.take(1)
    send(squares.at[x], squares.at[x], mate, square_slot)
    arrive(squares.at[1 - x], square_slot)
    width = 2 * wide
    mean = (own_squares + squares[1 - x][:, :1]) / width
    tokens[z, x] = (after[...] * lax.rsqrt(mean + epsilon) * norm_gain[...]).astype(BF16)

    def column_tokens(z_):
        return tokens.at[z_, x]

    token_z = slots.take(Z_CHIPS - 1)
    token_x = slots.take(Z_CHIPS)

    def cross(z_, i):
        send(column_tokens(z_), column_tokens(z_), mate, token_x + i)

    relayed = []

    def collect(j, when):
        z_ = (z_in, z_out)[j]

        @pl.when(when)
        def _():
            arrive(column_tokens(z_), token_z + 1 + j)

        copy = send(column_tokens(z_), column_tokens(z_), near, token_z + 1 + j, when & is_inner,
                    when is is_outer)
        if when is is_inner:
            relayed.append(copy)
        send(column_tokens(z_), column_tokens(z_), mate, token_x + 2 + j, when)

    multicast(column_tokens, token_z)
    cross(z, 0)
    deal(downs, down_chunk, NEAR)
    deal(downs, down_chunk, MID)
    ups.spread(FAR, is_outer)
    ups.spread(MID, is_outer)
    arrive(column_tokens(z_near), token_z)
    cross(z_near, 1)
    collect(0, is_inner)
    collect(1, is_inner)
    down_own.wait()
    downs.spread(OWN)
    for k in (NEAR, FAR, MID):
        ups.pass_on(k)
    collect(0, is_outer)
    for k in range(Z_CHIPS):
        ups.wait_twin(k)

    halves = up_all.shape[0] // 2

    def up_rows(i):
        return up_all[i * halves : (i + 1) * halves].reshape(wide, chunk)

    def activate(pair):
        first = pl.ds(2 * pair, 2)
        hidden = jnp.dot(
            tokens[first, 0].reshape(2 * rows, wide), up_rows(0), preferred_element_type=F32
        ) + jnp.dot(
            tokens[first, 1].reshape(2 * rows, wide), up_rows(1), preferred_element_type=F32
        )
        act[first] = jnp.square(jnp.maximum(hidden, 0.0)).astype(BF16).reshape(2, rows, chunk)

    span = parts.shape[3]
    early_kept, early_sent = x == half, x != half
    part_slot = slots.take(2 * Z_CHIPS)
    pairs = (half, 1 - half)
    visits = ((z_near, z), (z_in, z_out))

    def project(group, i):
        pair = pl.ds(2 * pairs[i], 2)
        cols = down_all[:, pl.ds(pl.multiple_of(group * span, span), span)]
        product = jnp.dot(act[pair].reshape(2 * rows, chunk), cols, preferred_element_type=F32)
        parts[group, pair] = product.astype(BF16).reshape(2, rows, span)

    def hand_over(group, i, when):
        a = group % 2
        for z_ in visits[i]:
            send(parts.at[group, z_], parts_in.at[a, z_], mate, part_slot + a * Z_CHIPS + z_, when)

    for i, z_ in enumerate((z, z_near)):
        arrive(tokens.at[z_, 1 - x], token_x + i)
    activate(half)
    for copy in relayed:
        pl.when(is_inner)(lambda: copy().wait_send())
    deal(downs, down_chunk, FAR, is_inner)
    downs.spread(NEAR, is_outer)
    collect(1, is_outer)
    deal(downs, down_chunk, FAR, is_outer)
    downs.pass_on(OWN)
    downs.wait_twin(OWN)
    project(z, 0)
    hand_over(z, 0, early_sent)
    for k in (NEAR, MID, FAR):
        downs.spread(k, is_inner)
    for i, z_ in ((2, z_in), (3, z_out)):
        arrive(tokens.at[z_, 1 - x], token_x + i)
    activate(1 - half)
    project(z, 1)
    hand_over(z, 1, early_sent)

    sum_slot = slots.take(4 * 2)

    def both(a, z_):
        arrive(parts_in.at[a, z_], part_slot + a * Z_CHIPS + z_)
        return parts[2 * x + a, z_].astype(F32) + parts_in[a, z_].astype(F32)

    def settle_own(a, when):
        @pl.when(when)
        def _():
            cols = pl.ds(pl.multiple_of(a * span, span), span)
            after[:, cols] = after[:, cols] + both(a, z)

    def deliver(a, i, row, peer, when):
        send(sum_out.at[i, a], sum_in.at[row, a], peer, sum_slot + 2 * row + a, when)

    def settle_near(a, when):
        @pl.when(when)
        def _():
            sum_out[0, a] = both(a, z_near).astype(BF16)

        deliver(a, 0, 0, near, when)

    def settle_far(a, j, when):
        z_ = (z_in, z_out)[j]

        @pl.when(when & is_outer)
        def _():
            sum_out[1 + j, a] = both(a, z_).astype(BF16)

        deliver(a, 1 + j, 2 + j, near, when & is_outer)

        @pl.when(when & is_inner)
        def _():
            mine = both(a, z_)
            arrive(sum_in.at[2 + j, a], sum_slot + 2 * (2 + j) + a)
            sum_out[1 + j, a] = (mine + sum_in[2 + j, a].astype(F32)).astype(BF16)

        deliver(a, 1 + j, 1, (across, beyond)[j], when & is_inner)

    def settle(a, when):
        for j in range(2):
            settle_far(a, j, when)
        settle_near(a, when)
        settle_own(a, when)

    downs.spread(FAR, is_outer)
    downs.pass_on(NEAR)
    downs.wait_twin(NEAR)
    for i in (1, 0):
        project(z_near, i)
        hand_over(z_near, i, early_sent)
    downs.spread(MID, is_outer)
    downs.pass_on(FAR)
    downs.wait_twin(FAR)
    for i in (1, 0):
        project(z_out, i)
        hand_over(z_out, i, early_kept)
    downs.pass_on(MID)
    downs.wait_twin(MID)
    for i in (1, 0):
        project(z_in, i)
        hand_over(z_in, i, early_kept)
    settle(half, early_kept)
    settle(1 - half, early_kept)
    settle(z_out % 2, early_sent)
    settle(z_in % 2, early_sent)

    for row in range(2):
        for a in range(2):
            arrive(sum_in.at[row, a], sum_slot + 2 * row + a)
    for a in range(2):
        cols = slice(a * span, (a + 1) * span)
        total = after[:, cols] + sum_in[0, a].astype(F32) + sum_in[1, a].astype(F32)
        out[:, cols] = total.astype(out.dtype)
    for copy, when in started:
        if when is None:
            copy().wait_send()
        else:
            pl.when(when)(lambda: copy().wait_send())


def on_chip(sp_size, residual, queries, key_proj, value_proj, diff_lambda, head_gain, out_weight,
            norm_gain, up_weight, down_weight):
    rows, wide = residual.shape
    kw = key_proj.shape[1] // KV_HEADS
    chunk = up_weight.shape[1] // Z_CHIPS
    span = sp_size // Z_CHIPS * down_weight.shape[1]
    hbm = pl.BlockSpec(memory_space=pltpu.HBM)
    vmem = pl.BlockSpec(memory_space=pltpu.VMEM)
    smem = pl.BlockSpec(memory_space=pltpu.SMEM)
    copies = 160
    return pl.pallas_call(
        fused_kernel,
        out_shape=jax.ShapeDtypeStruct(residual.shape, BF16),
        in_specs=[hbm, hbm, hbm, hbm, smem, vmem, hbm, vmem, hbm, hbm],
        out_specs=vmem,
        scratch_shapes=[
            pltpu.VMEM((sp_size, 2 * key_proj.shape[0], 2 * kw), BF16),
            pltpu.VMEM((sp_size, up_weight.shape[0], chunk), BF16),
            pltpu.VMEM((chunk, sp_size * down_weight.shape[1]), BF16),
            pltpu.VMEM(queries.shape, BF16),
            pltpu.VMEM(residual.shape, BF16),
            pltpu.VMEM(out_weight.shape, BF16),
            pltpu.VMEM((2, rows, wide), BF16),
            pltpu.VMEM((2, rows, 128), F32),
            pltpu.VMEM((Z_CHIPS, 2, rows, wide), BF16),
            pltpu.VMEM((Z_CHIPS, rows, chunk), BF16),
            pltpu.VMEM((Z_CHIPS, Z_CHIPS, rows, span), BF16),
            pltpu.VMEM((2, Z_CHIPS, rows, span), BF16),
            pltpu.VMEM((3, 2, rows, span), BF16),
            pltpu.VMEM((4, 2, rows, span), BF16),
            pltpu.VMEM((rows, wide), F32),
            pltpu.SemaphoreType.DMA((8,)),
            pltpu.SemaphoreType.DMA((copies,)),
            pltpu.SemaphoreType.DMA((copies,)),
        ],
        compiler_params=pltpu.CompilerParams(
            collective_id=0, has_side_effects=True, vmem_limit_bytes=60 * 2**20
        ),
        name="fused_layer",
    )(residual, queries, key_proj, value_proj, diff_lambda, head_gain.reshape(1, -1), out_weight,
      norm_gain.reshape(1, -1), up_weight, down_weight)


def solution(mesh):
    sp_size, tp_size = mesh.shape["sp"], mesh.shape["tp"]
    direct = tp_size == KV_HEADS == 2 and sp_size == Z_CHIPS * Y_CHIPS * CHIP_CORES
    body = functools.partial(on_chip, sp_size) if direct else on_device
    return jax.shard_map(
        body,
        mesh=mesh,
        in_specs=(
            P("sp", "tp"),
            P("sp", "tp"),
            P(("sp", "tp"), None),
            P(("sp", "tp"), None),
            P(),
            P(),
            P(None, "tp"),
            P("tp"),
            P("sp", "tp"),
            P("tp", "sp"),
        ),
        out_specs=P("sp", "tp"),
        check_vma=False,
    )
```

```python
import functools
import math

import jax
import jax.numpy as jnp
from jax import lax
from jax.experimental import pallas as pl
from jax.experimental.pallas import tpu as pltpu
from jax.sharding import PartitionSpec as P

D = 2048
HEADS = 8
KV_HEADS = 2
HEAD_DIM = 128
VALUE_DIM = 256


epsilon = 1e-06


def head_norm(per_map, lambdas, gain):
    difference = per_map[:, 0] - lambdas[:, None, None] * per_map[:, 1]
    scaled = (
        difference
        * lax.rsqrt(jnp.mean(difference * difference, axis=-1, keepdims=True) + epsilon)
        * gain
    )
    return scaled.astype(jnp.bfloat16)


def on_device(
    residual,
    queries,
    key_proj,
    value_proj,
    diff_lambda,
    head_gain,
    out_weight,
    norm_gain,
    up_weight,
    down_weight,
):
    rows_here = residual.shape[0]
    per_group = HEADS // KV_HEADS
    scaling = HEAD_DIM ** (-0.5)
    all_queries = lax.all_gather(queries, "tp", axis=1, tiled=True)
    query_grid = all_queries.reshape(rows_here, KV_HEADS, per_group, 2, HEAD_DIM)
    stat_shape = (KV_HEADS, per_group, 2, rows_here)
    maxima = jnp.full(stat_shape, -1e30, jnp.float32)
    key_piece = lax.all_gather(key_proj, "sp", axis=0, tiled=True)
    value_piece = lax.all_gather(value_proj, "sp", axis=0, tiled=True)
    key_count = key_piece.shape[0]
    key_grid = key_piece.reshape(key_count, KV_HEADS, 2, HEAD_DIM)
    value_grid = value_piece.reshape(key_count, KV_HEADS, VALUE_DIM)
    scores = (
        jnp.einsum("qagcd,kacd->agcqk", query_grid, key_grid, preferred_element_type=jnp.float32)
        * scaling
    )
    highest = jnp.maximum(maxima, jnp.max(scores, axis=-1))
    weights = jnp.exp(scores - highest[..., None])
    totals = jnp.sum(weights, axis=-1)
    weighted = jnp.einsum(
        "agcqk,kae->agcqe",
        weights.astype(jnp.bfloat16),
        value_grid,
        preferred_element_type=jnp.float32,
    )
    maxima, totals, weighted = (highest, totals, weighted)
    maxima = maxima.reshape(HEADS, 2, rows_here)
    totals = totals.reshape(HEADS, 2, rows_here)
    weighted = weighted.reshape(HEADS, 2, rows_here, VALUE_DIM)
    tp_size = lax.axis_size("tp")
    local_heads = HEADS // tp_size
    got_max, got_tot, got_sum = (
        lax.all_to_all(maxima, "tp", split_axis=0, concat_axis=0, tiled=True),
        lax.all_to_all(totals, "tp", split_axis=0, concat_axis=0, tiled=True),
        lax.all_to_all(weighted, "tp", split_axis=0, concat_axis=0, tiled=True),
    )
    got_max = got_max.reshape(tp_size, local_heads, 2, rows_here)
    got_tot = got_tot.reshape(tp_size, local_heads, 2, rows_here)
    got_sum = got_sum.reshape(tp_size, local_heads, 2, rows_here, VALUE_DIM)
    highest = jnp.max(got_max, axis=0)
    factor = jnp.exp(got_max - highest)
    totals_all = jnp.sum(factor * got_tot, axis=0)
    sums_all = jnp.sum(factor[..., None] * got_sum, axis=0)
    lambdas = lax.dynamic_slice_in_dim(diff_lambda, lax.axis_index("tp") * local_heads, local_heads)
    own_heads = head_norm(sums_all / totals_all[..., None], lambdas, head_gain)
    head_outputs = lax.all_gather(own_heads, "tp", axis=0, tiled=True)
    out_grid = out_weight.reshape(HEADS, VALUE_DIM, out_weight.shape[1])
    projected = jnp.einsum(
        "hqe,hed->qd", head_outputs, out_grid, preferred_element_type=jnp.float32
    )
    after_mix = residual.astype(jnp.float32) + projected
    squares = lax.psum(jnp.sum(after_mix * after_mix, axis=1), "tp")
    normed = (after_mix * lax.rsqrt(squares / D + epsilon)[:, None] * norm_gain).astype(
        jnp.bfloat16
    )
    full_rows = lax.all_gather(normed, "tp", axis=1, tiled=True)
    hidden = jnp.dot(
        full_rows,
        lax.all_gather(up_weight, "sp", axis=0, tiled=True),
        preferred_element_type=jnp.float32,
    )
    activated = jnp.square(jax.nn.relu(hidden)).astype(jnp.bfloat16)
    partial_value = jnp.dot(
        activated,
        lax.all_gather(down_weight, "sp", axis=1, tiled=True),
        preferred_element_type=jnp.float32,
    )
    mixer_sum = lax.psum_scatter(partial_value, "tp", scatter_dimension=1, tiled=True)
    return (after_mix + mixer_sum).astype(jnp.bfloat16)


MESH = pl.DeviceIdType.MESH
F32 = jnp.float32
BF16 = jnp.bfloat16
CHIP_CORES = 2
Y_CHIPS = 2
Z_CHIPS = 4
OWN, NEAR, FAR, MID = range(Z_CHIPS)


class Slots:
    def __init__(self):
        self.used = 0

    def take(self, count):
        base = self.used
        self.used += count
        return base


def fused_kernel(
    residual, queries, keys, values, lambdas, head_gain, out_weight, norm_gain,
    up, down, out,
    kv_all, up_all, down_all, q_buf, res_buf, w_buf, heads_all, squares, tokens, act,
    parts, parts_in, sum_out, sum_in, after, local_sem, send_sem, recv_sem,
):
    x = lax.axis_index("tp")
    s = lax.axis_index("sp")
    core, y, z = s % CHIP_CORES, (s // CHIP_CORES) % Y_CHIPS, s // (CHIP_CORES * Y_CHIPS)

    def place(z_, y_, c_):
        return (z_ * Y_CHIPS + y_) * CHIP_CORES + c_

    half = z // 2
    inner = ((z + 1) // 2) % 2
    z_near = 4 * half + 1 - z
    z_in, z_out = 2 - half, 3 - 3 * half
    is_inner, is_outer = inner == 1, inner == 0
    same = 1 - (x + half) % 2
    sends_far, keeps_far = same == 1, same == 0

    def in_column(z_):
        return {"sp": place(z_, y, core), "tp": x}

    mate = {"sp": s, "tp": 1 - x}
    beside = {"sp": place(z, 1 - y, core), "tp": x}
    twin = {"sp": place(z, y, 1 - core), "tp": x}
    near, across, beyond = in_column(z_near), in_column(z_in), in_column(z_out)

    barrier = pltpu.get_barrier_semaphore()
    peers = [mate, beside, twin, near, across, beyond]
    for peer in peers:
        pl.semaphore_signal(barrier, inc=1, device_id=peer, device_id_type=MESH)

    count = {"local": 0, "remote": 0}
    slots = Slots()
    started = []

    def bring(src, dst):
        copy = pltpu.make_async_copy(src, dst, local_sem.at[count["local"]])
        count["local"] += 1
        copy.start()
        return copy

    def send(src, dst, peer, slot, when=None, waits=True):
        i = count["remote"]
        count["remote"] += 1

        def copy():
            return pltpu.make_async_remote_copy(
                src_ref=src, dst_ref=dst, send_sem=send_sem.at[i], recv_sem=recv_sem.at[slot],
                device_id=peer, device_id_type=MESH,
            )

        if when is None:
            copy().start()
        else:
            pl.when(when)(lambda: copy().start())
        if waits:
            started.append((copy, when))
        return copy

    def arrive(dst, slot, when=None):
        if when is not None:
            pl.when(when)(lambda: arrive(dst, slot))
            return
        pltpu.make_async_remote_copy(
            src_ref=dst, dst_ref=dst, send_sem=send_sem.at[0], recv_sem=recv_sem.at[slot],
            device_id=mate, device_id_type=MESH,
        ).wait_recv()

    few = keys.shape[0]
    kw = kv_all.shape[2] // 2
    chunk = up_all.shape[2]
    lanes = down.shape[1]

    def half_of(ref, part):
        return ref.at[:, pl.ds(pl.multiple_of(part * kw, kw), kw)]

    def kv_rows(block, part, side):
        return kv_all.at[block, pl.ds(pl.multiple_of(part * few, few), few), pl.ds(side * kw, kw)]

    own_kv = [bring(half_of(keys, x), kv_rows(s, x, 0)), bring(half_of(values, x), kv_rows(s, x, 1))]
    q_copy = bring(queries, q_buf)

    pl.semaphore_wait(barrier, len(peers))

    swap = slots.take(2)
    for side, ref in enumerate((keys, values)):
        send(half_of(ref, 1 - x), kv_rows(s, x, side), mate, swap + side)
    w_copy = bring(out_weight, w_buf)
    r_copy = bring(residual, res_buf)

    def up_chunk(part):
        return up.at[:, pl.ds(pl.multiple_of(part * chunk, chunk), chunk)]

    def down_chunk(part):
        return down.at[pl.ds(pl.multiple_of(part * chunk, chunk), chunk), :]

    def kv_block(b):
        return kv_all.at[b]

    def up_block(b):
        return up_all.at[b]

    def down_block(b):
        return down_all.at[:, pl.ds(pl.multiple_of(b * lanes, lanes), lanes)]

    up_own = bring(up_chunk(z), up_block(s))
    down_own = bring(down_chunk(z), down_block(s))

    def relay(block, base, j):
        z_ = (z_in, z_out)[j]
        send(block(z_), block(z_), near, base + 1 + j, is_inner)

    class Stream:
        def __init__(self, block_of, order):
            self.block_of, self.order = block_of, list(order)
            self.z, self.y, self.twin, self.far = (slots.take(Z_CHIPS) for _ in range(4))

        def block(self, k, y_, c_):
            return self.block_of(place(self.order[k], y_, c_))

        def spread(self, k, when=None):
            b = self.block(k, y, core)
            if k != OWN:
                arrive(b, self.z + k, when)
            send(b, b, beside, self.y + k, when)
            send(b, b, twin, self.twin + k, when)

        def pass_on(self, k):
            b = self.block(k, 1 - y, core)
            arrive(b, self.y + k)
            send(b, b, twin, self.far + k)

        def wait_twin(self, k, side=None):
            if side != 1:
                arrive(self.block(k, y, 1 - core), self.twin + k)
            if side != 0:
                arrive(self.block(k, 1 - y, 1 - core), self.far + k)

    kv = Stream(kv_block, (z, z_near, z_in, z_out))
    ups = Stream(up_block, (z, z_near, z_out, z_in))
    downs = Stream(down_block, (
        z,
        same * z_out + (1 - same) * z_near,
        same * z_in + (1 - same) * z_out,
        same * z_near + (1 - same) * z_in,
    ))

    def deal(stream, piece_of, k, when=None):
        z_, peer, slot = {
            NEAR: (z_near, near, NEAR), FAR: (z_out, beyond, FAR + inner), MID: (z_in, across, FAR + inner),
        }[k]
        if stream is downs:
            theirs = same if k == NEAR else 1 - same
            slot = 1 + (slot - 1 + 2 * theirs) % 3
        send(piece_of(z_), stream.block_of(s), peer, stream.z + slot, when)

    def kv_onward(k):
        b = kv.block(k, y, core)
        send(b, b, beside, kv.y + k)
        send(b, b, twin, kv.twin + k)

    def column_kv(z_):
        return kv_block(place(z_, y, core))

    outlets = (
        (beside, kv.y), (twin, kv.twin), (near, kv.z + 1), (across, kv.z + 3 - inner)
    )
    for peer, slot in outlets:
        for side, ref in enumerate((keys, values)):
            send(half_of(ref, x), kv_rows(s, x, side), peer, slot)
    for side in range(2):
        arrive(kv_rows(s, 1 - x, side), swap + side)
    mates_rows = kv_all.at[s, pl.ds(pl.multiple_of((1 - x) * few, few), few), :]
    for peer, slot in outlets:
        send(mates_rows, mates_rows, peer, slot)
    deal(ups, up_chunk, NEAR, is_outer)
    deal(ups, up_chunk, MID)
    kv.spread(1)
    arrive(kv.block(2, y, core), kv.z + 2)
    relay(column_kv, kv.z + 1, 0)
    arrive(kv.block(3, y, core), kv.z + 3, is_inner)
    relay(column_kv, kv.z + 1, 1)
    deal(ups, up_chunk, NEAR, is_inner)
    kv_onward(2)
    arrive(kv.block(3, y, core), kv.z + 3, is_outer)
    deal(ups, up_chunk, FAR)
    kv_onward(3)
    up_own.wait()
    ups.spread(OWN)
    for copy in own_kv:
        copy.wait()
    for k in range(Z_CHIPS):
        kv.pass_on(k)
    for k in range(Z_CHIPS):
        kv.wait_twin(k)
    q_copy.wait()

    local_heads = q_buf.shape[1] // (2 * HEAD_DIM)
    blocks, per_block = kv_all.shape[0], kv_all.shape[1]
    key_count = blocks * per_block
    factor = HEAD_DIM ** (-0.5) * math.log2(math.e)
    vals = lambda: kv_all[:, :, kw:].reshape(key_count, kw)
    heads = slots.take(local_heads)

    def head_cols(part, h):
        return heads_all.at[part, :, pl.ds(h * VALUE_DIM, VALUE_DIM)]

    for h in range(local_heads):
        maps = []
        for c in range(2):
            q = q_buf[:, (2 * h + c) * HEAD_DIM : (2 * h + c + 1) * HEAD_DIM]
            k = kv_all[:, :, c * HEAD_DIM : (c + 1) * HEAD_DIM].reshape(key_count, HEAD_DIM)
            scores = lax.dot_general(q, k, (((1,), (1,)), ((), ())), preferred_element_type=F32)
            top = jnp.max(scores, axis=1, keepdims=True)
            weights = jnp.exp2((scores - top) * factor)
            total = jnp.sum(weights, axis=1, keepdims=True)
            summed = jnp.dot(weights.astype(BF16), vals(), preferred_element_type=F32)
            maps.append(summed / total)
        diff = maps[0] - lambdas[x * local_heads + h] * maps[1]
        scaled = diff * lax.rsqrt(jnp.mean(diff * diff, axis=1, keepdims=True) + epsilon)
        heads_all[x, :, pl.ds(h * VALUE_DIM, VALUE_DIM)] = (scaled * head_gain[...]).astype(BF16)
        send(head_cols(x, h), head_cols(x, h), mate, heads + h)
        if h < 2:
            ups.spread((NEAR, FAR)[h], is_inner)
    ups.spread(MID, is_inner)
    ups.spread(NEAR, is_outer)
    ups.pass_on(OWN)

    wide = heads_all.shape[2]
    rows = heads_all.shape[1]
    w_copy.wait()
    r_copy.wait()

    def w_rows(part):
        return w_buf[pl.ds(pl.multiple_of(part * wide, wide), wide), :]

    mix = res_buf[...].astype(F32) + jnp.dot(heads_all[x], w_rows(x), preferred_element_type=F32)
    for h in range(local_heads):
        arrive(head_cols(1 - x, h), heads + h)
    mix = mix + jnp.dot(heads_all[1 - x], w_rows(1 - x), preferred_element_type=F32)
    after[...] = mix
    own_squares = jnp.sum(mix * mix, axis=1, keepdims=True)
    width = 2 * wide
    tokens[z, x] = (mix * norm_gain[...]).astype(BF16)
    squares[z, x] = jnp.broadcast_to(own_squares, (rows, rows)).T[: squares.shape[2]]

    token_z = slots.take(2 * (Z_CHIPS - 1))
    token_x = slots.take(2 * Z_CHIPS)

    def send_tokens(z_, peer, slot, when=None, waits=True):
        return [
            send(ref.at[z_, x], ref.at[z_, x], peer, slot + n, when, waits)
            for n, ref in enumerate((tokens, squares))
        ]

    def take_tokens(z_, part, slot, when=None):
        for n, ref in enumerate((tokens, squares)):
            arrive(ref.at[z_, part], slot + n, when)

    relayed = []

    def collect(j, when):
        z_ = (z_in, z_out)[j]
        take_tokens(z_, x, token_z + 2 + 2 * j, when)
        if when is is_inner:
            relayed.extend(send_tokens(z_, near, token_z + 2 + 2 * j, when, False))
        send_tokens(z_, mate, token_x + 4 + 2 * j, when)

    send_tokens(z, near, token_z)
    send_tokens(z, across, token_z + 4 - 2 * inner)
    send_tokens(z, mate, token_x)
    deal(downs, down_chunk, NEAR, is_outer | keeps_far)
    deal(downs, down_chunk, MID)
    ups.spread(FAR, is_outer)
    ups.spread(MID, is_outer)
    take_tokens(z_near, x, token_z)
    send_tokens(z_near, mate, token_x + 2)
    collect(0, is_inner)
    collect(1, is_inner)
    deal(downs, down_chunk, NEAR, is_inner & sends_far)
    down_own.wait()
    downs.spread(OWN)
    for k in (NEAR, FAR, MID):
        ups.pass_on(k)
    collect(0, is_outer)
    for k in range(Z_CHIPS):
        ups.wait_twin(k)

    halves = up_all.shape[0] // 2

    def up_rows(i):
        return up_all[i * halves : (i + 1) * halves].reshape(wide, chunk)

    def activate(pair):
        first = pl.ds(2 * pair, 2)
        hidden = jnp.dot(
            tokens[first, 0].reshape(2 * rows, wide), up_rows(0), preferred_element_type=F32
        ) + jnp.dot(
            tokens[first, 1].reshape(2 * rows, wide), up_rows(1), preferred_element_type=F32
        )
        factors = []
        for i in range(2):
            mean = (squares[2 * pair + i, 0] + squares[2 * pair + i, 1])[:1] / width
            factors.append(jnp.broadcast_to(lax.rsqrt(mean + epsilon), (rows, rows)).T[:, :1])
        hidden = hidden * jnp.concatenate(factors, axis=0)
        act[first] = jnp.square(jnp.maximum(hidden, 0.0)).astype(BF16).reshape(2, rows, chunk)

    span = parts.shape[3]
    part_slot = slots.take(2 * Z_CHIPS)
    pairs = (pl.ds(2 * half, 2), pl.ds(2 * (1 - half), 2))
    sides = (y, 1 - y)

    def project(k, side, i, when=None):
        unit = Y_CHIPS * downs.order[k] + sides[side]
        cols = down_all[:, pl.ds(pl.multiple_of(unit * span, span), span)]
        product = jnp.dot(
            act[pairs[i]].reshape(2 * rows, chunk), cols, preferred_element_type=F32
        )
        parts[unit, pairs[i]] = product.astype(BF16).reshape(2, rows, span)
        if when is not False:
            kept = unit % Z_CHIPS
            send(parts.at[unit, pairs[i]], parts_in.at[kept, pairs[i]], mate,
                 part_slot + 2 * kept + i, when)

    for i, z_ in enumerate((z, z_near)):
        take_tokens(z_, 1 - x, token_x + 2 * i)
    activate(half)
    for copy in relayed:
        pl.when(is_inner)(lambda: copy().wait_send())
    deal(downs, down_chunk, FAR, is_inner)
    downs.wait_twin(OWN, 0)
    project(OWN, 0, 0, keeps_far)
    downs.spread(1, is_inner | keeps_far)
    collect(1, is_outer)
    deal(downs, down_chunk, FAR, is_outer)
    downs.pass_on(OWN)
    downs.wait_twin(OWN, 1)
    project(OWN, 1, 0, keeps_far)
    downs.spread(2, is_inner)
    downs.spread(3, is_inner)
    downs.spread(1, is_outer & sends_far)
    downs.wait_twin(1, 0)
    project(1, 0, 0)
    for i, z_ in ((2, z_in), (3, z_out)):
        take_tokens(z_, 1 - x, token_x + 2 * i)
    activate(1 - half)
    for side in range(2):
        project(OWN, side, 1, keeps_far)
    project(1, 0, 1)
    downs.spread(2, is_outer)
    downs.pass_on(1)
    downs.wait_twin(1, 1)
    for i in (1, 0):
        project(1, 1, i)
    downs.wait_twin(2, 0)
    for i in (1, 0):
        project(2, 0, i, sends_far)
    downs.spread(3, is_outer)
    downs.pass_on(2)
    downs.wait_twin(2, 1)
    for i in (1, 0):
        project(2, 1, i, sends_far)

    sum_slot = slots.take(4 * Z_CHIPS)

    def deliver(i, u, row, peer, when):
        send(sum_out.at[i, u], sum_in.at[row, u], peer, sum_slot + Z_CHIPS * row + u, when)

    def both(u, z_):
        return parts[Z_CHIPS * x + u, z_].astype(F32) + parts_in[u, z_].astype(F32)

    def settle_far(u, when):
        arrive(parts_in.at[u, pairs[1]], part_slot + 2 * u + 1, when)
        for j, z_ in enumerate((z_in, z_out)):

            @pl.when(when & is_outer)
            def _():
                sum_out[1 + j, u] = both(u, z_).astype(BF16)

            deliver(1 + j, u, 2 + j, near, when & is_outer)

            @pl.when(when & is_inner)
            def _():
                mine = both(u, z_)
                arrive(sum_in.at[2 + j, u], sum_slot + Z_CHIPS * (2 + j) + u)
                sum_out[1 + j, u] = (mine + sum_in[2 + j, u].astype(F32)).astype(BF16)

            deliver(1 + j, u, 1, (across, beyond)[j], when & is_inner)

    def settle_half(u, when):
        arrive(parts_in.at[u, pairs[0]], part_slot + 2 * u, when)

        @pl.when(when)
        def _():
            sum_out[0, u] = both(u, z_near).astype(BF16)

        deliver(0, u, 0, near, when)

        @pl.when(when)
        def _():
            cols = pl.ds(pl.multiple_of(u * span, span), span)
            after[:, cols] = after[:, cols] + both(u, z)

    def columns(a):
        return [Y_CHIPS * a + side for side in sides]

    outer_sends, inner_sends = sends_far & is_outer, sends_far & is_inner
    for u in columns(half):
        settle_far(u, outer_sends)
    downs.wait_twin(3, 0)
    for i in (1, 0):
        project(3, 0, i, False)
    downs.pass_on(3)
    downs.wait_twin(3, 1)
    for i in (1, 0):
        project(3, 1, i, False)
    for u in columns(1 - half):
        settle_far(u, outer_sends)
        settle_half(u, inner_sends)
    for u in columns(half):
        settle_half(u, outer_sends)
        settle_far(u, inner_sends)
        settle_half(u, inner_sends)
    for u in columns(1 - half):
        settle_half(u, outer_sends)
        settle_far(u, inner_sends)
    for u in columns(z_out % 2) + columns(z_in % 2):
        settle_far(u, keeps_far & is_outer)
        settle_half(u, keeps_far)
        settle_far(u, keeps_far & is_inner)

    for row in range(2):
        for u in range(Z_CHIPS):
            arrive(sum_in.at[row, u], sum_slot + Z_CHIPS * row + u)
    for u in range(Z_CHIPS):
        cols = slice(u * span, (u + 1) * span)
        total = after[:, cols] + sum_in[0, u].astype(F32) + sum_in[1, u].astype(F32)
        out[:, cols] = total.astype(out.dtype)
    for copy, when in started:
        if when is None:
            copy().wait_send()
        else:
            pl.when(when)(lambda: copy().wait_send())


def on_chip(sp_size, residual, queries, key_proj, value_proj, diff_lambda, head_gain, out_weight,
            norm_gain, up_weight, down_weight):
    rows, wide = residual.shape
    kw = key_proj.shape[1] // KV_HEADS
    chunk = up_weight.shape[1] // Z_CHIPS
    span = CHIP_CORES * down_weight.shape[1]
    units = Z_CHIPS * Y_CHIPS
    hbm = pl.BlockSpec(memory_space=pltpu.HBM)
    vmem = pl.BlockSpec(memory_space=pltpu.VMEM)
    smem = pl.BlockSpec(memory_space=pltpu.SMEM)
    copies = 256
    return pl.pallas_call(
        fused_kernel,
        out_shape=jax.ShapeDtypeStruct(residual.shape, BF16),
        in_specs=[hbm, hbm, hbm, hbm, smem, vmem, hbm, vmem, hbm, hbm],
        out_specs=vmem,
        scratch_shapes=[
            pltpu.VMEM((sp_size, 2 * key_proj.shape[0], 2 * kw), BF16),
            pltpu.VMEM((sp_size, up_weight.shape[0], chunk), BF16),
            pltpu.VMEM((chunk, sp_size * down_weight.shape[1]), BF16),
            pltpu.VMEM(queries.shape, BF16),
            pltpu.VMEM(residual.shape, BF16),
            pltpu.VMEM(out_weight.shape, BF16),
            pltpu.VMEM((2, rows, wide), BF16),
            pltpu.VMEM((Z_CHIPS, 2, 8, rows), F32),
            pltpu.VMEM((Z_CHIPS, 2, rows, wide), BF16),
            pltpu.VMEM((Z_CHIPS, rows, chunk), BF16),
            pltpu.VMEM((units, Z_CHIPS, rows, span), BF16),
            pltpu.VMEM((units // 2, Z_CHIPS, rows, span), BF16),
            pltpu.VMEM((3, units // 2, rows, span), BF16),
            pltpu.VMEM((4, units // 2, rows, span), BF16),
            pltpu.VMEM((rows, wide), F32),
            pltpu.SemaphoreType.DMA((8,)),
            pltpu.SemaphoreType.DMA((copies,)),
            pltpu.SemaphoreType.DMA((copies,)),
        ],
        compiler_params=pltpu.CompilerParams(
            collective_id=0, has_side_effects=True, vmem_limit_bytes=60 * 2**20
        ),
        name="fused_layer",
    )(residual, queries, key_proj, value_proj, diff_lambda, head_gain.reshape(1, -1), out_weight,
      norm_gain.reshape(1, -1), up_weight, down_weight)


def solution(mesh):
    sp_size, tp_size = mesh.shape["sp"], mesh.shape["tp"]
    direct = tp_size == KV_HEADS == 2 and sp_size == Z_CHIPS * Y_CHIPS * CHIP_CORES
    body = functools.partial(on_chip, sp_size) if direct else on_device
    return jax.shard_map(
        body,
        mesh=mesh,
        in_specs=(
            P("sp", "tp"),
            P("sp", "tp"),
            P(("sp", "tp"), None),
            P(("sp", "tp"), None),
            P(),
            P(),
            P(None, "tp"),
            P("tp"),
            P("sp", "tp"),
            P("tp", "sp"),
        ),
        out_specs=P("sp", "tp"),
        check_vma=False,
    )
```

```python
import functools
import math

import jax
import jax.numpy as jnp
from jax import lax
from jax.experimental import pallas as pl
from jax.experimental.pallas import tpu as pltpu
from jax.sharding import PartitionSpec as P

D = 2048
HEADS = 8
KV_HEADS = 2
HEAD_DIM = 128
VALUE_DIM = 256


epsilon = 1e-06


def head_norm(per_map, lambdas, gain):
    difference = per_map[:, 0] - lambdas[:, None, None] * per_map[:, 1]
    scaled = (
        difference
        * lax.rsqrt(jnp.mean(difference * difference, axis=-1, keepdims=True) + epsilon)
        * gain
    )
    return scaled.astype(jnp.bfloat16)


def on_device(
    residual,
    queries,
    key_proj,
    value_proj,
    diff_lambda,
    head_gain,
    out_weight,
    norm_gain,
    up_weight,
    down_weight,
):
    rows_here = residual.shape[0]
    per_group = HEADS // KV_HEADS
    scaling = HEAD_DIM ** (-0.5)
    all_queries = lax.all_gather(queries, "tp", axis=1, tiled=True)
    query_grid = all_queries.reshape(rows_here, KV_HEADS, per_group, 2, HEAD_DIM)
    stat_shape = (KV_HEADS, per_group, 2, rows_here)
    maxima = jnp.full(stat_shape, -1e30, jnp.float32)
    key_piece = lax.all_gather(key_proj, "sp", axis=0, tiled=True)
    value_piece = lax.all_gather(value_proj, "sp", axis=0, tiled=True)
    key_count = key_piece.shape[0]
    key_grid = key_piece.reshape(key_count, KV_HEADS, 2, HEAD_DIM)
    value_grid = value_piece.reshape(key_count, KV_HEADS, VALUE_DIM)
    scores = (
        jnp.einsum("qagcd,kacd->agcqk", query_grid, key_grid, preferred_element_type=jnp.float32)
        * scaling
    )
    highest = jnp.maximum(maxima, jnp.max(scores, axis=-1))
    weights = jnp.exp(scores - highest[..., None])
    totals = jnp.sum(weights, axis=-1)
    weighted = jnp.einsum(
        "agcqk,kae->agcqe",
        weights.astype(jnp.bfloat16),
        value_grid,
        preferred_element_type=jnp.float32,
    )
    maxima, totals, weighted = (highest, totals, weighted)
    maxima = maxima.reshape(HEADS, 2, rows_here)
    totals = totals.reshape(HEADS, 2, rows_here)
    weighted = weighted.reshape(HEADS, 2, rows_here, VALUE_DIM)
    tp_size = lax.axis_size("tp")
    local_heads = HEADS // tp_size
    got_max, got_tot, got_sum = (
        lax.all_to_all(maxima, "tp", split_axis=0, concat_axis=0, tiled=True),
        lax.all_to_all(totals, "tp", split_axis=0, concat_axis=0, tiled=True),
        lax.all_to_all(weighted, "tp", split_axis=0, concat_axis=0, tiled=True),
    )
    got_max = got_max.reshape(tp_size, local_heads, 2, rows_here)
    got_tot = got_tot.reshape(tp_size, local_heads, 2, rows_here)
    got_sum = got_sum.reshape(tp_size, local_heads, 2, rows_here, VALUE_DIM)
    highest = jnp.max(got_max, axis=0)
    factor = jnp.exp(got_max - highest)
    totals_all = jnp.sum(factor * got_tot, axis=0)
    sums_all = jnp.sum(factor[..., None] * got_sum, axis=0)
    lambdas = lax.dynamic_slice_in_dim(diff_lambda, lax.axis_index("tp") * local_heads, local_heads)
    own_heads = head_norm(sums_all / totals_all[..., None], lambdas, head_gain)
    head_outputs = lax.all_gather(own_heads, "tp", axis=0, tiled=True)
    out_grid = out_weight.reshape(HEADS, VALUE_DIM, out_weight.shape[1])
    projected = jnp.einsum(
        "hqe,hed->qd", head_outputs, out_grid, preferred_element_type=jnp.float32
    )
    after_mix = residual.astype(jnp.float32) + projected
    squares = lax.psum(jnp.sum(after_mix * after_mix, axis=1), "tp")
    normed = (after_mix * lax.rsqrt(squares / D + epsilon)[:, None] * norm_gain).astype(
        jnp.bfloat16
    )
    full_rows = lax.all_gather(normed, "tp", axis=1, tiled=True)
    hidden = jnp.dot(
        full_rows,
        lax.all_gather(up_weight, "sp", axis=0, tiled=True),
        preferred_element_type=jnp.float32,
    )
    activated = jnp.square(jax.nn.relu(hidden)).astype(jnp.bfloat16)
    partial_value = jnp.dot(
        activated,
        lax.all_gather(down_weight, "sp", axis=1, tiled=True),
        preferred_element_type=jnp.float32,
    )
    mixer_sum = lax.psum_scatter(partial_value, "tp", scatter_dimension=1, tiled=True)
    return (after_mix + mixer_sum).astype(jnp.bfloat16)


MESH = pl.DeviceIdType.MESH
F32 = jnp.float32
BF16 = jnp.bfloat16
CHIP_CORES = 2
Y_CHIPS = 2
Z_CHIPS = 4
OWN, NEAR, FAR, MID = range(Z_CHIPS)


class Slots:
    def __init__(self):
        self.used = 0

    def take(self, count):
        base = self.used
        self.used += count
        return base


def fused_kernel(
    residual, queries, keys, values, lambdas, head_gain, out_weight, norm_gain,
    up, down, out,
    kv_all, up_all, down_all, q_buf, res_buf, w_buf, heads_all, squares, tokens, act,
    parts, parts_in, sum_out, sum_in, after, local_sem, send_sem, recv_sem,
):
    x = lax.axis_index("tp")
    s = lax.axis_index("sp")
    core, y, z = s % CHIP_CORES, (s // CHIP_CORES) % Y_CHIPS, s // (CHIP_CORES * Y_CHIPS)

    def place(z_, y_, c_):
        return (z_ * Y_CHIPS + y_) * CHIP_CORES + c_

    half = z // 2
    inner = ((z + 1) // 2) % 2
    z_near = 4 * half + 1 - z
    z_in, z_out = 2 - half, 3 - 3 * half
    is_inner, is_outer = inner == 1, inner == 0
    same = 1 - (x + half) % 2
    sends_far, keeps_far = same == 1, same == 0

    def in_column(z_):
        return {"sp": place(z_, y, core), "tp": x}

    mate = {"sp": s, "tp": 1 - x}
    beside = {"sp": place(z, 1 - y, core), "tp": x}
    twin = {"sp": place(z, y, 1 - core), "tp": x}
    near, across, beyond = in_column(z_near), in_column(z_in), in_column(z_out)

    barrier = pltpu.get_barrier_semaphore()
    peers = [mate, beside, twin, near, across, beyond]
    for peer in peers:
        pl.semaphore_signal(barrier, inc=1, device_id=peer, device_id_type=MESH)

    local_copies = []
    slots = Slots()
    outgoing = {}

    def bring(src, dst):
        copy = pltpu.make_async_copy(src, dst, local_sem.at[len(local_copies)])
        local_copies.append(copy)
        copy.start()
        return copy

    def send(src, dst, peer, slot, group, when=None):
        i = outgoing.setdefault(group, len(outgoing))

        def start():
            pltpu.make_async_remote_copy(
                src_ref=src, dst_ref=dst, send_sem=send_sem.at[i], recv_sem=recv_sem.at[slot],
                device_id=peer, device_id_type=MESH,
            ).start()

        if when is None:
            start()
        else:
            pl.when(when)(start)

    def sent(group, whole, when=None):
        def wait():
            pltpu.make_async_remote_copy(
                src_ref=whole, dst_ref=whole, send_sem=send_sem.at[outgoing[group]],
                recv_sem=recv_sem.at[0], device_id=mate, device_id_type=MESH,
            ).wait_send()

        if when is None:
            wait()
        else:
            pl.when(when)(wait)

    def arrive(dst, slot, when=None):
        if when is not None:
            pl.when(when)(lambda: arrive(dst, slot))
            return
        pltpu.make_async_remote_copy(
            src_ref=dst, dst_ref=dst, send_sem=send_sem.at[0], recv_sem=recv_sem.at[slot],
            device_id=mate, device_id_type=MESH,
        ).wait_recv()

    few = keys.shape[0]
    kw = kv_all.shape[2] // 2
    chunk = up_all.shape[2]
    lanes = down.shape[1]

    def half_of(ref, part):
        return ref.at[:, pl.ds(pl.multiple_of(part * kw, kw), kw)]

    def kv_rows(block, part, side):
        return kv_all.at[block, pl.ds(pl.multiple_of(part * few, few), few), pl.ds(side * kw, kw)]

    own_kv = [bring(half_of(keys, x), kv_rows(s, x, 0)), bring(half_of(values, x), kv_rows(s, x, 1))]
    q_copy = bring(queries, q_buf)

    pl.semaphore_wait(barrier, len(peers))

    swap = slots.take(1)
    for side, ref in enumerate((keys, values)):
        send(half_of(ref, 1 - x), kv_rows(s, x, side), mate, swap, "swap")
    w_copy = bring(out_weight, w_buf)
    r_copy = bring(residual, res_buf)

    def up_chunk(part):
        return up.at[:, pl.ds(pl.multiple_of(part * chunk, chunk), chunk)]

    def down_chunk(part):
        return down.at[pl.ds(pl.multiple_of(part * chunk, chunk), chunk), :]

    def kv_block(b):
        return kv_all.at[b]

    def up_block(b):
        return up_all.at[b]

    def down_block(b):
        return down_all.at[:, pl.ds(pl.multiple_of(b * lanes, lanes), lanes)]

    up_own = bring(up_chunk(z), up_block(s))
    down_own = bring(down_chunk(z), down_block(s))

    def relay(block, base, j):
        z_ = (z_in, z_out)[j]
        send(block(z_), block(z_), near, base + 1 + j, "kv_relay", is_inner)

    class Stream:
        def __init__(self, name, block_of, order, staged=False):
            self.name, self.block_of, self.order = name, block_of, order
            self.z, self.y = slots.take(Z_CHIPS), slots.take(Z_CHIPS)
            self.step = int(staged)
            self.twin = slots.take(2 * Z_CHIPS if staged else 1)
            self.far = self.twin + Z_CHIPS * self.step

        def block(self, k, y_, c_):
            return self.block_of(place(self.order[k], y_, c_))

        def spread(self, k, when=None):
            b = self.block(k, y, core)
            if k != OWN:
                arrive(b, self.z + k, when)
            send(b, b, beside, self.y + k, self.name, when)
            send(b, b, twin, self.twin + k * self.step, self.name, when)

        def pass_on(self, k):
            b = self.block(k, 1 - y, core)
            arrive(b, self.y + k)
            send(b, b, twin, self.far + k * self.step, self.name)

        def wait_twin(self, k, side=None):
            if side != 1:
                arrive(self.block(k, y, 1 - core), self.twin + k)
            if side != 0:
                arrive(self.block(k, 1 - y, 1 - core), self.far + k)

    kv = Stream("kv", kv_block, (z, z_near, z_in, z_out))
    ups = Stream("up", up_block, (z, z_near, z_out, z_in))
    downs = Stream("down", down_block, (
        z,
        same * z_out + (1 - same) * z_near,
        same * z_in + (1 - same) * z_out,
        same * z_near + (1 - same) * z_in,
    ), staged=True)

    def deal(stream, piece_of, k, when=None):
        z_, peer, slot = {
            NEAR: (z_near, near, NEAR), FAR: (z_out, beyond, FAR + inner), MID: (z_in, across, FAR + inner),
        }[k]
        if stream is downs:
            theirs = same if k == NEAR else 1 - same
            slot = 1 + (slot - 1 + 2 * theirs) % 3
        send(piece_of(z_), stream.block_of(s), peer, stream.z + slot, stream.name, when)

    def kv_onward(k):
        b = kv.block(k, y, core)
        send(b, b, beside, kv.y + k, "kv")
        send(b, b, twin, kv.twin, "kv")

    def column_kv(z_):
        return kv_block(place(z_, y, core))

    outlets = (
        (beside, kv.y), (twin, kv.twin), (near, kv.z + 1), (across, kv.z + 3 - inner)
    )
    for peer, slot in outlets:
        for side, ref in enumerate((keys, values)):
            send(half_of(ref, x), kv_rows(s, x, side), peer, slot, "kv")
    mates_rows = kv_all.at[s, pl.ds(pl.multiple_of((1 - x) * few, few), few), :]
    arrive(mates_rows, swap)
    for peer, slot in outlets:
        send(mates_rows, mates_rows, peer, slot, "kv")
    deal(ups, up_chunk, NEAR, is_outer)
    deal(ups, up_chunk, MID)
    kv.spread(1)
    arrive(kv.block(2, y, core), kv.z + 2)
    relay(column_kv, kv.z + 1, 0)
    arrive(kv.block(3, y, core), kv.z + 3, is_inner)
    relay(column_kv, kv.z + 1, 1)
    deal(ups, up_chunk, NEAR, is_inner)
    kv_onward(2)
    arrive(kv.block(3, y, core), kv.z + 3, is_outer)
    deal(ups, up_chunk, FAR)
    kv_onward(3)
    up_own.wait()
    ups.spread(OWN)
    for copy in own_kv:
        copy.wait()
    for k in range(Z_CHIPS):
        kv.pass_on(k)
    arrive(kv_all.at[pl.ds(0, 2 * Z_CHIPS)], kv.twin)
    q_copy.wait()

    local_heads = q_buf.shape[1] // (2 * HEAD_DIM)
    blocks, per_block = kv_all.shape[0], kv_all.shape[1]
    key_count = blocks * per_block
    factor = HEAD_DIM ** (-0.5) * math.log2(math.e)
    vals = lambda: kv_all[:, :, kw:].reshape(key_count, kw)
    heads = slots.take(1)

    def head_cols(part, h):
        return heads_all.at[part, :, pl.ds(h * VALUE_DIM, VALUE_DIM)]

    for h in range(local_heads):
        maps = []
        for c in range(2):
            q = q_buf[:, (2 * h + c) * HEAD_DIM : (2 * h + c + 1) * HEAD_DIM]
            k = kv_all[:, :, c * HEAD_DIM : (c + 1) * HEAD_DIM].reshape(key_count, HEAD_DIM)
            scores = lax.dot_general(q, k, (((1,), (1,)), ((), ())), preferred_element_type=F32)
            top = jnp.max(scores, axis=1, keepdims=True)
            weights = jnp.exp2((scores - top) * factor)
            total = jnp.sum(weights, axis=1, keepdims=True)
            summed = jnp.dot(weights.astype(BF16), vals(), preferred_element_type=F32)
            maps.append(summed / total)
        diff = maps[0] - lambdas[x * local_heads + h] * maps[1]
        scaled = diff * lax.rsqrt(jnp.mean(diff * diff, axis=1, keepdims=True) + epsilon)
        heads_all[x, :, pl.ds(h * VALUE_DIM, VALUE_DIM)] = (scaled * head_gain[...]).astype(BF16)
        send(head_cols(x, h), head_cols(x, h), mate, heads, "heads")
        if h < 2:
            ups.spread((NEAR, FAR)[h], is_inner)
    ups.spread(MID, is_inner)
    ups.spread(NEAR, is_outer)
    ups.pass_on(OWN)

    wide = heads_all.shape[2]
    rows = heads_all.shape[1]
    w_copy.wait()
    r_copy.wait()

    def w_rows(part):
        return w_buf[pl.ds(pl.multiple_of(part * wide, wide), wide), :]

    mix = res_buf[...].astype(F32) + jnp.dot(heads_all[x], w_rows(x), preferred_element_type=F32)
    arrive(heads_all.at[1 - x], heads)
    mix = mix + jnp.dot(heads_all[1 - x], w_rows(1 - x), preferred_element_type=F32)
    after[...] = mix
    own_squares = jnp.sum(mix * mix, axis=1, keepdims=True)
    width = 2 * wide
    tokens[z, x] = (mix * norm_gain[...]).astype(BF16)
    squares[z, x] = jnp.broadcast_to(own_squares, (rows, rows)).T[: squares.shape[2]]

    token_z = slots.take(2 * (Z_CHIPS - 1))
    token_x = slots.take(2 * Z_CHIPS)

    def send_tokens(z_, peer, slot, when=None, group="token"):
        for n, ref in enumerate((tokens, squares)):
            send(ref.at[z_, x], ref.at[z_, x], peer, slot + n, (group, n), when)

    def take_tokens(z_, part, slot, when=None):
        for n, ref in enumerate((tokens, squares)):
            arrive(ref.at[z_, part], slot + n, when)

    def collect(j, when):
        z_ = (z_in, z_out)[j]
        take_tokens(z_, x, token_z + 2 + 2 * j, when)
        if when is is_inner:
            send_tokens(z_, near, token_z + 2 + 2 * j, when, "relay")
        send_tokens(z_, mate, token_x + 4 + 2 * j, when)

    send_tokens(z, near, token_z)
    send_tokens(z, across, token_z + 4 - 2 * inner)
    send_tokens(z, mate, token_x)
    deal(downs, down_chunk, NEAR, is_outer | keeps_far)
    deal(downs, down_chunk, MID)
    ups.spread(FAR, is_outer)
    ups.spread(MID, is_outer)
    down_own.wait()
    downs.spread(OWN)
    take_tokens(z_near, x, token_z)
    send_tokens(z_near, mate, token_x + 2)
    collect(0, is_inner)
    collect(1, is_inner)
    deal(downs, down_chunk, NEAR, is_inner & sends_far)
    for k in (NEAR, FAR, MID):
        ups.pass_on(k)
    collect(0, is_outer)
    deal(downs, down_chunk, FAR, is_outer)
    arrive(up_all.at[pl.ds(0, 2 * Z_CHIPS)], ups.twin)

    halves = up_all.shape[0] // 2

    def up_rows(i):
        return up_all[i * halves : (i + 1) * halves].reshape(wide, chunk)

    def activate(pair):
        first = pl.ds(2 * pair, 2)
        hidden = jnp.dot(
            tokens[first, 0].reshape(2 * rows, wide), up_rows(0), preferred_element_type=F32
        ) + jnp.dot(
            tokens[first, 1].reshape(2 * rows, wide), up_rows(1), preferred_element_type=F32
        )
        factors = []
        for i in range(2):
            mean = (squares[2 * pair + i, 0] + squares[2 * pair + i, 1])[:1] / width
            factors.append(jnp.broadcast_to(lax.rsqrt(mean + epsilon), (rows, rows)).T[:, :1])
        hidden = hidden * jnp.concatenate(factors, axis=0)
        act[first] = jnp.square(jnp.maximum(hidden, 0.0)).astype(BF16).reshape(2, rows, chunk)

    span = parts.shape[3]
    part_slot = slots.take(2 * Z_CHIPS)
    pairs = (pl.ds(2 * half, 2), pl.ds(2 * (1 - half), 2))
    sides = (y, 1 - y)

    def project(k, side, i, when=None):
        unit = Y_CHIPS * downs.order[k] + sides[side]
        cols = down_all[:, pl.ds(pl.multiple_of(unit * span, span), span)]
        product = jnp.dot(
            act[pairs[i]].reshape(2 * rows, chunk), cols, preferred_element_type=F32
        )
        parts[unit, pairs[i]] = product.astype(BF16).reshape(2, rows, span)
        if when is not False:
            kept = unit % Z_CHIPS
            send(parts.at[unit, pairs[i]], parts_in.at[kept, pairs[i]], mate,
                 part_slot + 2 * kept + i, "parts", when)

    for i, z_ in enumerate((z, z_near)):
        take_tokens(z_, 1 - x, token_x + 2 * i)
    activate(half)
    sent(("relay", 0), tokens.at[0], is_inner)
    sent(("relay", 1), squares.at[0], is_inner)
    deal(downs, down_chunk, FAR, is_inner)
    downs.wait_twin(OWN, 0)
    project(OWN, 0, 0, keeps_far)
    downs.spread(1, is_inner | keeps_far)
    collect(1, is_outer)
    downs.pass_on(OWN)
    downs.wait_twin(OWN, 1)
    project(OWN, 1, 0, keeps_far)
    downs.spread(2, is_inner)
    downs.spread(3, is_inner)
    downs.spread(1, is_outer & sends_far)
    downs.wait_twin(1, 0)
    project(1, 0, 0)
    for i, z_ in ((2, z_in), (3, z_out)):
        take_tokens(z_, 1 - x, token_x + 2 * i)
    activate(1 - half)
    for side in range(2):
        project(OWN, side, 1, keeps_far)
    project(1, 0, 1)
    downs.spread(2, is_outer)
    downs.pass_on(1)
    downs.wait_twin(1, 1)
    for i in (1, 0):
        project(1, 1, i)
    downs.wait_twin(2, 0)
    for i in (1, 0):
        project(2, 0, i, sends_far)
    downs.spread(3, is_outer)
    downs.pass_on(2)
    downs.wait_twin(2, 1)
    for i in (1, 0):
        project(2, 1, i, sends_far)

    sum_slot, pass_slot = slots.take(2), slots.take(2 * Z_CHIPS)

    def deliver(i, u, row, peer, when):
        slot = sum_slot + row if row < 2 else pass_slot + Z_CHIPS * (row - 2) + u
        send(sum_out.at[i, u], sum_in.at[row, u], peer, slot, "sums", when)

    def both(u, z_):
        return parts[Z_CHIPS * x + u, z_].astype(F32) + parts_in[u, z_].astype(F32)

    def settle_far(u, when):
        arrive(parts_in.at[u, pairs[1]], part_slot + 2 * u + 1, when)
        for j, z_ in enumerate((z_in, z_out)):

            @pl.when(when & is_outer)
            def _():
                sum_out[1 + j, u] = both(u, z_).astype(BF16)

            deliver(1 + j, u, 2 + j, near, when & is_outer)

            @pl.when(when & is_inner)
            def _():
                mine = both(u, z_)
                arrive(sum_in.at[2 + j, u], pass_slot + Z_CHIPS * j + u)
                sum_out[1 + j, u] = (mine + sum_in[2 + j, u].astype(F32)).astype(BF16)

            deliver(1 + j, u, 1, (across, beyond)[j], when & is_inner)

    def settle_half(u, when):
        arrive(parts_in.at[u, pairs[0]], part_slot + 2 * u, when)

        @pl.when(when)
        def _():
            sum_out[0, u] = both(u, z_near).astype(BF16)

        deliver(0, u, 0, near, when)

        @pl.when(when)
        def _():
            cols = pl.ds(pl.multiple_of(u * span, span), span)
            after[:, cols] = after[:, cols] + both(u, z)

    def columns(a):
        return [Y_CHIPS * a + side for side in sides]

    outer_sends, inner_sends = sends_far & is_outer, sends_far & is_inner
    for u in columns(half):
        settle_far(u, outer_sends)
    downs.wait_twin(3, 0)
    for i in (1, 0):
        project(3, 0, i, False)
    downs.pass_on(3)
    downs.wait_twin(3, 1)
    for i in (1, 0):
        project(3, 1, i, False)
    for u in columns(1 - half):
        settle_far(u, outer_sends)
        settle_half(u, inner_sends)
    for u in columns(half):
        settle_half(u, outer_sends)
        settle_far(u, inner_sends)
        settle_half(u, inner_sends)
    for u in columns(1 - half):
        settle_half(u, outer_sends)
        settle_far(u, inner_sends)
    for u in columns(z_out % 2) + columns(z_in % 2):
        settle_far(u, keeps_far & is_outer)
        settle_half(u, keeps_far)
        settle_far(u, keeps_far & is_inner)

    for group, whole in (
        ("swap", kv_all.at[0, pl.ds(0, few), :]),
        ("kv", kv_all.at[pl.ds(0, 3 * Z_CHIPS + 2)]),
        ("up", up_all.at[pl.ds(0, 4 * Z_CHIPS - 1)]),
        ("down", down_all.at[:, pl.ds(0, (4 * Z_CHIPS - 1) * lanes)]),
        ("heads", heads_all.at[0]),
        (("token", 0), tokens.at[pl.ds(0, 3)]),
        (("token", 1), squares.at[pl.ds(0, 3)]),
        ("parts", parts.at[pl.ds(0, Z_CHIPS)]),
    ):
        sent(group, whole)
    sent("kv_relay", kv_all.at[pl.ds(0, 2)], is_inner)
    for row in range(2):
        arrive(sum_in.at[row], sum_slot + row)
    for u in range(Z_CHIPS):
        cols = slice(u * span, (u + 1) * span)
        total = after[:, cols] + sum_in[0, u].astype(F32) + sum_in[1, u].astype(F32)
        out[:, cols] = total.astype(out.dtype)
    sent("sums", sum_out)
    assert slots.used <= recv_sem.shape[0] and len(outgoing) <= send_sem.shape[0]


def on_chip(sp_size, residual, queries, key_proj, value_proj, diff_lambda, head_gain, out_weight,
            norm_gain, up_weight, down_weight):
    rows, wide = residual.shape
    kw = key_proj.shape[1] // KV_HEADS
    chunk = up_weight.shape[1] // Z_CHIPS
    span = CHIP_CORES * down_weight.shape[1]
    units = Z_CHIPS * Y_CHIPS
    hbm = pl.BlockSpec(memory_space=pltpu.HBM)
    vmem = pl.BlockSpec(memory_space=pltpu.VMEM)
    smem = pl.BlockSpec(memory_space=pltpu.SMEM)
    receives, groups = 68, 12
    return pl.pallas_call(
        fused_kernel,
        out_shape=jax.ShapeDtypeStruct(residual.shape, BF16),
        in_specs=[hbm, hbm, hbm, hbm, smem, vmem, hbm, vmem, hbm, hbm],
        out_specs=vmem,
        scratch_shapes=[
            pltpu.VMEM((sp_size, 2 * key_proj.shape[0], 2 * kw), BF16),
            pltpu.VMEM((sp_size, up_weight.shape[0], chunk), BF16),
            pltpu.VMEM((chunk, sp_size * down_weight.shape[1]), BF16),
            pltpu.VMEM(queries.shape, BF16),
            pltpu.VMEM(residual.shape, BF16),
            pltpu.VMEM(out_weight.shape, BF16),
            pltpu.VMEM((2, rows, wide), BF16),
            pltpu.VMEM((Z_CHIPS, 2, 8, rows), F32),
            pltpu.VMEM((Z_CHIPS, 2, rows, wide), BF16),
            pltpu.VMEM((Z_CHIPS, rows, chunk), BF16),
            pltpu.VMEM((units, Z_CHIPS, rows, span), BF16),
            pltpu.VMEM((units // 2, Z_CHIPS, rows, span), BF16),
            pltpu.VMEM((3, units // 2, rows, span), BF16),
            pltpu.VMEM((4, units // 2, rows, span), BF16),
            pltpu.VMEM((rows, wide), F32),
            pltpu.SemaphoreType.DMA((7,)),
            pltpu.SemaphoreType.DMA((groups,)),
            pltpu.SemaphoreType.DMA((receives,)),
        ],
        compiler_params=pltpu.CompilerParams(
            collective_id=0, has_side_effects=True, vmem_limit_bytes=60 * 2**20
        ),
        name="fused_layer",
    )(residual, queries, key_proj, value_proj, diff_lambda, head_gain.reshape(1, -1), out_weight,
      norm_gain.reshape(1, -1), up_weight, down_weight)


def solution(mesh):
    sp_size, tp_size = mesh.shape["sp"], mesh.shape["tp"]
    direct = tp_size == KV_HEADS == 2 and sp_size == Z_CHIPS * Y_CHIPS * CHIP_CORES
    body = functools.partial(on_chip, sp_size) if direct else on_device
    return jax.shard_map(
        body,
        mesh=mesh,
        in_specs=(
            P("sp", "tp"),
            P("sp", "tp"),
            P(("sp", "tp"), None),
            P(("sp", "tp"), None),
            P(),
            P(),
            P(None, "tp"),
            P("tp"),
            P("sp", "tp"),
            P("tp", "sp"),
        ),
        out_specs=P("sp", "tp"),
        check_vma=False,
    )
```

```python
import functools
import math

import jax
import jax.numpy as jnp
from jax import lax
from jax.experimental import pallas as pl
from jax.experimental.pallas import tpu as pltpu
from jax.sharding import PartitionSpec as P

D = 2048
HEADS = 8
KV_HEADS = 2
HEAD_DIM = 128
VALUE_DIM = 256


epsilon = 1e-06


def head_norm(per_map, lambdas, gain):
    difference = per_map[:, 0] - lambdas[:, None, None] * per_map[:, 1]
    scaled = (
        difference
        * lax.rsqrt(jnp.mean(difference * difference, axis=-1, keepdims=True) + epsilon)
        * gain
    )
    return scaled.astype(jnp.bfloat16)


def on_device(
    residual,
    queries,
    key_proj,
    value_proj,
    diff_lambda,
    head_gain,
    out_weight,
    norm_gain,
    up_weight,
    down_weight,
):
    rows_here = residual.shape[0]
    per_group = HEADS // KV_HEADS
    scaling = HEAD_DIM ** (-0.5)
    all_queries = lax.all_gather(queries, "tp", axis=1, tiled=True)
    query_grid = all_queries.reshape(rows_here, KV_HEADS, per_group, 2, HEAD_DIM)
    stat_shape = (KV_HEADS, per_group, 2, rows_here)
    maxima = jnp.full(stat_shape, -1e30, jnp.float32)
    key_piece = lax.all_gather(key_proj, "sp", axis=0, tiled=True)
    value_piece = lax.all_gather(value_proj, "sp", axis=0, tiled=True)
    key_count = key_piece.shape[0]
    key_grid = key_piece.reshape(key_count, KV_HEADS, 2, HEAD_DIM)
    value_grid = value_piece.reshape(key_count, KV_HEADS, VALUE_DIM)
    scores = (
        jnp.einsum("qagcd,kacd->agcqk", query_grid, key_grid, preferred_element_type=jnp.float32)
        * scaling
    )
    highest = jnp.maximum(maxima, jnp.max(scores, axis=-1))
    weights = jnp.exp(scores - highest[..., None])
    totals = jnp.sum(weights, axis=-1)
    weighted = jnp.einsum(
        "agcqk,kae->agcqe",
        weights.astype(jnp.bfloat16),
        value_grid,
        preferred_element_type=jnp.float32,
    )
    maxima, totals, weighted = (highest, totals, weighted)
    maxima = maxima.reshape(HEADS, 2, rows_here)
    totals = totals.reshape(HEADS, 2, rows_here)
    weighted = weighted.reshape(HEADS, 2, rows_here, VALUE_DIM)
    tp_size = lax.axis_size("tp")
    local_heads = HEADS // tp_size
    got_max, got_tot, got_sum = (
        lax.all_to_all(maxima, "tp", split_axis=0, concat_axis=0, tiled=True),
        lax.all_to_all(totals, "tp", split_axis=0, concat_axis=0, tiled=True),
        lax.all_to_all(weighted, "tp", split_axis=0, concat_axis=0, tiled=True),
    )
    got_max = got_max.reshape(tp_size, local_heads, 2, rows_here)
    got_tot = got_tot.reshape(tp_size, local_heads, 2, rows_here)
    got_sum = got_sum.reshape(tp_size, local_heads, 2, rows_here, VALUE_DIM)
    highest = jnp.max(got_max, axis=0)
    factor = jnp.exp(got_max - highest)
    totals_all = jnp.sum(factor * got_tot, axis=0)
    sums_all = jnp.sum(factor[..., None] * got_sum, axis=0)
    lambdas = lax.dynamic_slice_in_dim(diff_lambda, lax.axis_index("tp") * local_heads, local_heads)
    own_heads = head_norm(sums_all / totals_all[..., None], lambdas, head_gain)
    head_outputs = lax.all_gather(own_heads, "tp", axis=0, tiled=True)
    out_grid = out_weight.reshape(HEADS, VALUE_DIM, out_weight.shape[1])
    projected = jnp.einsum(
        "hqe,hed->qd", head_outputs, out_grid, preferred_element_type=jnp.float32
    )
    after_mix = residual.astype(jnp.float32) + projected
    squares = lax.psum(jnp.sum(after_mix * after_mix, axis=1), "tp")
    normed = (after_mix * lax.rsqrt(squares / D + epsilon)[:, None] * norm_gain).astype(
        jnp.bfloat16
    )
    full_rows = lax.all_gather(normed, "tp", axis=1, tiled=True)
    hidden = jnp.dot(
        full_rows,
        lax.all_gather(up_weight, "sp", axis=0, tiled=True),
        preferred_element_type=jnp.float32,
    )
    activated = jnp.square(jax.nn.relu(hidden)).astype(jnp.bfloat16)
    partial_value = jnp.dot(
        activated,
        lax.all_gather(down_weight, "sp", axis=1, tiled=True),
        preferred_element_type=jnp.float32,
    )
    mixer_sum = lax.psum_scatter(partial_value, "tp", scatter_dimension=1, tiled=True)
    return (after_mix + mixer_sum).astype(jnp.bfloat16)


MESH = pl.DeviceIdType.MESH
F32 = jnp.float32
BF16 = jnp.bfloat16
CHIP_CORES = 2
Y_CHIPS = 2
Z_CHIPS = 4
OWN, NEAR, FAR, MID = range(Z_CHIPS)


class Slots:
    def __init__(self):
        self.used = 0

    def take(self, count):
        base = self.used
        self.used += count
        return base


def fused_kernel(
    residual, queries, keys, values, lambdas, head_gain, out_weight, norm_gain,
    up, down, out,
    kv_all, up_all, down_all, q_buf, res_buf, w_buf, heads_all, squares, tokens, act,
    parts, parts_in, sum_out, sum_in, after, local_sem, send_sem, recv_sem, go,
):
    x = lax.axis_index("tp")
    s = lax.axis_index("sp")
    core, y, z = s % CHIP_CORES, (s // CHIP_CORES) % Y_CHIPS, s // (CHIP_CORES * Y_CHIPS)

    def place(z_, y_, c_):
        return (z_ * Y_CHIPS + y_) * CHIP_CORES + c_

    half = z // 2
    inner = ((z + 1) // 2) % 2
    z_near = 4 * half + 1 - z
    z_in, z_out = 2 - half, 3 - 3 * half
    is_inner, is_outer = inner == 1, inner == 0
    same = 1 - (x + half) % 2
    sends_far, keeps_far = same == 1, same == 0

    def in_column(z_):
        return {"sp": place(z_, y, core), "tp": x}

    mate = {"sp": s, "tp": 1 - x}
    beside = {"sp": place(z, 1 - y, core), "tp": x}
    twin = {"sp": place(z, y, 1 - core), "tp": x}
    near, across, beyond = in_column(z_near), in_column(z_in), in_column(z_out)

    barrier = pltpu.get_barrier_semaphore()
    peers = [mate, beside, twin, near, across, beyond]
    for peer in peers:
        pl.semaphore_signal(barrier, inc=1, device_id=peer, device_id_type=MESH)

    local_copies = []
    slots = Slots()
    outgoing = {}

    def bring(src, dst):
        copy = pltpu.make_async_copy(src, dst, local_sem.at[len(local_copies)])
        local_copies.append(copy)
        copy.start()
        return copy

    def send(src, dst, peer, slot, group, when=None):
        i = outgoing.setdefault(group, len(outgoing))

        def start():
            pltpu.make_async_remote_copy(
                src_ref=src, dst_ref=dst, send_sem=send_sem.at[i], recv_sem=recv_sem.at[slot],
                device_id=peer, device_id_type=MESH,
            ).start()

        if when is None:
            start()
        else:
            pl.when(when)(start)

    def sent(group, whole, when=None):
        def wait():
            pltpu.make_async_remote_copy(
                src_ref=whole, dst_ref=whole, send_sem=send_sem.at[outgoing[group]],
                recv_sem=recv_sem.at[0], device_id=mate, device_id_type=MESH,
            ).wait_send()

        if when is None:
            wait()
        else:
            pl.when(when)(wait)

    def arrive(dst, slot, when=None):
        if when is not None:
            pl.when(when)(lambda: arrive(dst, slot))
            return
        pltpu.make_async_remote_copy(
            src_ref=dst, dst_ref=dst, send_sem=send_sem.at[0], recv_sem=recv_sem.at[slot],
            device_id=mate, device_id_type=MESH,
        ).wait_recv()

    few = keys.shape[0]
    kw = kv_all.shape[2] // 2
    chunk = up_all.shape[2]
    lanes = down.shape[1]

    def half_of(ref, part):
        return ref.at[:, pl.ds(pl.multiple_of(part * kw, kw), kw)]

    def kv_rows(block, part, side):
        return kv_all.at[block, pl.ds(pl.multiple_of(part * few, few), few), pl.ds(side * kw, kw)]

    own_kv = [bring(half_of(keys, x), kv_rows(s, x, 0)), bring(half_of(values, x), kv_rows(s, x, 1))]
    q_copy = bring(queries, q_buf)

    pl.semaphore_wait(barrier, len(peers))

    swap = slots.take(1)
    for side, ref in enumerate((keys, values)):
        send(half_of(ref, 1 - x), kv_rows(s, x, side), mate, swap, "swap")
    w_copy = bring(out_weight, w_buf)
    r_copy = bring(residual, res_buf)

    def up_chunk(part):
        return up.at[:, pl.ds(pl.multiple_of(part * chunk, chunk), chunk)]

    def down_chunk(part):
        return down.at[pl.ds(pl.multiple_of(part * chunk, chunk), chunk), :]

    def kv_block(b):
        return kv_all.at[b]

    def up_block(b):
        return up_all.at[b]

    def down_block(b):
        return down_all.at[:, pl.ds(pl.multiple_of(b * lanes, lanes), lanes)]

    up_own = bring(up_chunk(z), up_block(s))
    down_own = bring(down_chunk(z), down_block(s))

    def relay(block, base, j):
        z_ = (z_in, z_out)[j]
        send(block(z_), block(z_), near, base + 1 + j, "kv_relay", is_inner)

    class Stream:
        def __init__(self, name, block_of, order, staged=False):
            self.name, self.block_of, self.order = name, block_of, order
            self.z, self.y = slots.take(Z_CHIPS), slots.take(Z_CHIPS)
            self.step = int(staged)
            self.twin = slots.take(2 * Z_CHIPS if staged else 1)
            self.far = self.twin + Z_CHIPS * self.step

        def block(self, k, y_, c_):
            return self.block_of(place(self.order[k], y_, c_))

        def spread(self, k, when=None):
            b = self.block(k, y, core)
            if k != OWN:
                arrive(b, self.z + k, when)
            send(b, b, beside, self.y + k, self.name, when)
            send(b, b, twin, self.twin + k * self.step, self.name, when)

        def pass_on(self, k):
            b = self.block(k, 1 - y, core)
            arrive(b, self.y + k)
            send(b, b, twin, self.far + k * self.step, self.name)

        def wait_twin(self, k, side=None):
            if side != 1:
                arrive(self.block(k, y, 1 - core), self.twin + k)
            if side != 0:
                arrive(self.block(k, 1 - y, 1 - core), self.far + k)

    kv = Stream("kv", kv_block, (z, z_near, z_in, z_out))
    ups = Stream("up", up_block, (z, z_near, z_out, z_in))
    downs = Stream("down", down_block, (
        z,
        same * z_out + (1 - same) * z_near,
        same * z_in + (1 - same) * z_out,
        same * z_near + (1 - same) * z_in,
    ), staged=True)

    def deal(stream, piece_of, k, when=None):
        z_, peer, slot = {
            NEAR: (z_near, near, NEAR), FAR: (z_out, beyond, FAR + inner), MID: (z_in, across, FAR + inner),
        }[k]
        if stream is downs:
            theirs = same if k == NEAR else 1 - same
            slot = 1 + (slot - 1 + 2 * theirs) % 3
        send(piece_of(z_), stream.block_of(s), peer, stream.z + slot, stream.name, when)

    def kv_onward(k):
        b = kv.block(k, y, core)
        send(b, b, beside, kv.y + k, "kv")
        send(b, b, twin, kv.twin, "kv")

    def column_kv(z_):
        return kv_block(place(z_, y, core))

    outlets = (
        (beside, kv.y), (twin, kv.twin), (near, kv.z + 1), (across, kv.z + 3 - inner)
    )
    for peer, slot in outlets:
        for side, ref in enumerate((keys, values)):
            send(half_of(ref, x), kv_rows(s, x, side), peer, slot, "kv")
    mates_rows = kv_all.at[s, pl.ds(pl.multiple_of((1 - x) * few, few), few), :]
    arrive(mates_rows, swap)
    for peer, slot in outlets:
        send(mates_rows, mates_rows, peer, slot, "kv")
    deal(ups, up_chunk, NEAR, is_outer)
    deal(ups, up_chunk, MID)
    kv.spread(1)
    arrive(kv.block(2, y, core), kv.z + 2)
    relay(column_kv, kv.z + 1, 0)
    arrive(kv.block(3, y, core), kv.z + 3, is_inner)
    relay(column_kv, kv.z + 1, 1)
    deal(ups, up_chunk, NEAR, is_inner)
    kv_onward(2)
    arrive(kv.block(3, y, core), kv.z + 3, is_outer)
    deal(ups, up_chunk, FAR)
    kv_onward(3)
    up_own.wait()
    ups.spread(OWN)
    for copy in own_kv:
        copy.wait()
    for k in range(Z_CHIPS):
        kv.pass_on(k)
    arrive(kv_all.at[pl.ds(0, 2 * Z_CHIPS)], kv.twin)
    q_copy.wait()

    local_heads = q_buf.shape[1] // (2 * HEAD_DIM)
    blocks, per_block = kv_all.shape[0], kv_all.shape[1]
    key_count = blocks * per_block
    factor = HEAD_DIM ** (-0.5) * math.log2(math.e)
    vals = lambda: kv_all[:, :, kw:].reshape(key_count, kw)
    heads = slots.take(1)

    def head_cols(part, h):
        return heads_all.at[part, :, pl.ds(h * VALUE_DIM, VALUE_DIM)]

    for h in range(local_heads):
        maps = []
        for c in range(2):
            q = q_buf[:, (2 * h + c) * HEAD_DIM : (2 * h + c + 1) * HEAD_DIM]
            k = kv_all[:, :, c * HEAD_DIM : (c + 1) * HEAD_DIM].reshape(key_count, HEAD_DIM)
            scores = lax.dot_general(q, k, (((1,), (1,)), ((), ())), preferred_element_type=F32)
            top = jnp.max(scores, axis=1, keepdims=True)
            weights = jnp.exp2((scores - top) * factor)
            total = jnp.sum(weights, axis=1, keepdims=True)
            summed = jnp.dot(weights.astype(BF16), vals(), preferred_element_type=F32)
            maps.append(summed / total)
        diff = maps[0] - lambdas[x * local_heads + h] * maps[1]
        scaled = diff * lax.rsqrt(jnp.mean(diff * diff, axis=1, keepdims=True) + epsilon)
        heads_all[x, :, pl.ds(h * VALUE_DIM, VALUE_DIM)] = (scaled * head_gain[...]).astype(BF16)
        send(head_cols(x, h), head_cols(x, h), mate, heads, "heads")
        if h < 2:
            ups.spread((NEAR, FAR)[h], is_inner)
    ups.spread(MID, is_inner)
    ups.spread(NEAR, is_outer)
    ups.pass_on(OWN)

    wide = heads_all.shape[2]
    rows = heads_all.shape[1]
    w_copy.wait()
    r_copy.wait()

    def w_rows(part):
        return w_buf[pl.ds(pl.multiple_of(part * wide, wide), wide), :]

    mix = res_buf[...].astype(F32) + jnp.dot(heads_all[x], w_rows(x), preferred_element_type=F32)
    arrive(heads_all.at[1 - x], heads)
    mix = mix + jnp.dot(heads_all[1 - x], w_rows(1 - x), preferred_element_type=F32)
    after[...] = mix
    own_squares = jnp.sum(mix * mix, axis=1, keepdims=True)
    width = 2 * wide
    tokens[z, x] = (mix * norm_gain[...]).astype(BF16)
    squares[z, x] = jnp.broadcast_to(own_squares, (rows, rows)).T[: squares.shape[2]]

    token_z = slots.take(2 * (Z_CHIPS - 1))
    token_x = slots.take(2 * Z_CHIPS)

    def send_tokens(z_, peer, slot, when=None, group="token"):
        for n, ref in enumerate((tokens, squares)):
            send(ref.at[z_, x], ref.at[z_, x], peer, slot + n, (group, n), when)

    def take_tokens(z_, part, slot, when=None):
        for n, ref in enumerate((tokens, squares)):
            arrive(ref.at[z_, part], slot + n, when)

    def collect(j, when):
        z_ = (z_in, z_out)[j]
        take_tokens(z_, x, token_z + 2 + 2 * j, when)
        if when is is_inner:
            send_tokens(z_, near, token_z + 2 + 2 * j, when, "relay")
        send_tokens(z_, mate, token_x + 4 + 2 * j, when)

    send_tokens(z, near, token_z)
    send_tokens(z, across, token_z + 4 - 2 * inner)
    send_tokens(z, mate, token_x)
    deal(downs, down_chunk, NEAR, is_outer | keeps_far)
    deal(downs, down_chunk, MID)
    ups.spread(FAR, is_outer)
    ups.spread(MID, is_outer)
    down_own.wait()
    downs.spread(OWN)
    take_tokens(z_near, x, token_z)
    send_tokens(z_near, mate, token_x + 2)
    collect(0, is_inner)
    collect(1, is_inner)
    deal(downs, down_chunk, NEAR, is_inner & sends_far)
    for k in (NEAR, FAR, MID):
        ups.pass_on(k)
    collect(0, is_outer)
    arrive(up_all.at[pl.ds(0, 2 * Z_CHIPS)], ups.twin)

    halves = up_all.shape[0] // 2

    def up_rows(i):
        return up_all[i * halves : (i + 1) * halves].reshape(wide, chunk)

    def activate(pair):
        first = pl.ds(2 * pair, 2)
        hidden = jnp.dot(
            tokens[first, 0].reshape(2 * rows, wide), up_rows(0), preferred_element_type=F32
        ) + jnp.dot(
            tokens[first, 1].reshape(2 * rows, wide), up_rows(1), preferred_element_type=F32
        )
        factors = []
        for i in range(2):
            mean = (squares[2 * pair + i, 0] + squares[2 * pair + i, 1])[:1] / width
            factors.append(jnp.broadcast_to(lax.rsqrt(mean + epsilon), (rows, rows)).T[:, :1])
        hidden = hidden * jnp.concatenate(factors, axis=0)
        act[first] = jnp.square(jnp.maximum(hidden, 0.0)).astype(BF16).reshape(2, rows, chunk)

    span = parts.shape[3]
    part_slot = slots.take(2 * Z_CHIPS)
    pairs = (pl.ds(2 * half, 2), pl.ds(2 * (1 - half), 2))
    sides = (y, 1 - y)

    def project(k, side, i, when=None):
        unit = Y_CHIPS * downs.order[k] + sides[side]
        cols = down_all[:, pl.ds(pl.multiple_of(unit * span, span), span)]
        product = jnp.dot(
            act[pairs[i]].reshape(2 * rows, chunk), cols, preferred_element_type=F32
        )
        parts[unit, pairs[i]] = product.astype(BF16).reshape(2, rows, span)
        if when is not False:
            kept = unit % Z_CHIPS
            send(parts.at[unit, pairs[i]], parts_in.at[kept, pairs[i]], mate,
                 part_slot + 2 * kept + i, "parts", when)

    for i, z_ in enumerate((z, z_near)):
        take_tokens(z_, 1 - x, token_x + 2 * i)
    activate(half)
    sent(("relay", 0), tokens.at[0], is_inner)
    sent(("relay", 1), squares.at[0], is_inner)

    @pl.when(is_inner)
    def _():
        for peer in (across, beyond):
            pl.semaphore_signal(go, inc=1, device_id=peer, device_id_type=MESH)
        pl.semaphore_wait(go, 1)

    deal(downs, down_chunk, FAR, is_inner)
    downs.wait_twin(OWN, 0)
    project(OWN, 0, 0, keeps_far)
    downs.spread(1, is_inner | keeps_far)

    @pl.when(is_outer)
    def _():
        pl.semaphore_wait(go, 1)

    deal(downs, down_chunk, FAR, is_outer)
    collect(1, is_outer)
    downs.pass_on(OWN)
    downs.wait_twin(OWN, 1)
    project(OWN, 1, 0, keeps_far)
    downs.spread(2, is_inner)
    downs.spread(3, is_inner)
    downs.spread(1, is_outer & sends_far)
    downs.wait_twin(1, 0)
    project(1, 0, 0)
    for i, z_ in ((2, z_in), (3, z_out)):
        take_tokens(z_, 1 - x, token_x + 2 * i)
    activate(1 - half)
    for side in range(2):
        project(OWN, side, 1, keeps_far)
    project(1, 0, 1)
    downs.spread(2, is_outer)
    downs.pass_on(1)
    downs.wait_twin(1, 1)
    for i in (1, 0):
        project(1, 1, i)
    downs.wait_twin(2, 0)
    for i in (1, 0):
        project(2, 0, i, sends_far)
    downs.spread(3, is_outer)
    downs.pass_on(2)
    downs.wait_twin(2, 1)
    for i in (1, 0):
        project(2, 1, i, sends_far)

    sum_slot, pass_slot = slots.take(2), slots.take(2 * Z_CHIPS)

    def deliver(i, u, row, peer, when):
        slot = sum_slot + row if row < 2 else pass_slot + Z_CHIPS * (row - 2) + u
        send(sum_out.at[i, u], sum_in.at[row, u], peer, slot, "sums", when)

    def both(u, z_):
        return parts[Z_CHIPS * x + u, z_].astype(F32) + parts_in[u, z_].astype(F32)

    def settle_far(u, when):
        arrive(parts_in.at[u, pairs[1]], part_slot + 2 * u + 1, when)
        for j, z_ in enumerate((z_in, z_out)):

            @pl.when(when & is_outer)
            def _():
                sum_out[1 + j, u] = both(u, z_).astype(BF16)

            deliver(1 + j, u, 2 + j, near, when & is_outer)

            @pl.when(when & is_inner)
            def _():
                mine = both(u, z_)
                arrive(sum_in.at[2 + j, u], pass_slot + Z_CHIPS * j + u)
                sum_out[1 + j, u] = (mine + sum_in[2 + j, u].astype(F32)).astype(BF16)

            deliver(1 + j, u, 1, (across, beyond)[j], when & is_inner)

    def settle_half(u, when):
        arrive(parts_in.at[u, pairs[0]], part_slot + 2 * u, when)

        @pl.when(when)
        def _():
            sum_out[0, u] = both(u, z_near).astype(BF16)

        deliver(0, u, 0, near, when)

        @pl.when(when)
        def _():
            cols = pl.ds(pl.multiple_of(u * span, span), span)
            after[:, cols] = after[:, cols] + both(u, z)

    def columns(a):
        return [Y_CHIPS * a + side for side in sides]

    outer_sends, inner_sends = sends_far & is_outer, sends_far & is_inner
    for u in columns(half):
        settle_far(u, outer_sends)
    downs.wait_twin(3, 0)
    for i in (1, 0):
        project(3, 0, i, False)
    downs.pass_on(3)
    downs.wait_twin(3, 1)
    for i in (1, 0):
        project(3, 1, i, False)
    for u in columns(1 - half):
        settle_far(u, outer_sends)
        settle_half(u, inner_sends)
    for u in columns(half):
        settle_half(u, outer_sends)
        settle_far(u, inner_sends)
        settle_half(u, inner_sends)
    for u in columns(1 - half):
        settle_half(u, outer_sends)
        settle_far(u, inner_sends)
    for u in columns(z_out % 2) + columns(z_in % 2):
        settle_far(u, keeps_far & is_outer)
        settle_half(u, keeps_far)
        settle_far(u, keeps_far & is_inner)

    for group, whole in (
        ("swap", kv_all.at[0, pl.ds(0, few), :]),
        ("kv", kv_all.at[pl.ds(0, 3 * Z_CHIPS + 2)]),
        ("up", up_all.at[pl.ds(0, 4 * Z_CHIPS - 1)]),
        ("down", down_all.at[:, pl.ds(0, (4 * Z_CHIPS - 1) * lanes)]),
        ("heads", heads_all.at[0]),
        (("token", 0), tokens.at[pl.ds(0, 3)]),
        (("token", 1), squares.at[pl.ds(0, 3)]),
        ("parts", parts.at[pl.ds(0, Z_CHIPS)]),
    ):
        sent(group, whole)
    sent("kv_relay", kv_all.at[pl.ds(0, 2)], is_inner)
    for row in range(2):
        arrive(sum_in.at[row], sum_slot + row)
    for u in range(Z_CHIPS):
        cols = slice(u * span, (u + 1) * span)
        total = after[:, cols] + sum_in[0, u].astype(F32) + sum_in[1, u].astype(F32)
        out[:, cols] = total.astype(out.dtype)
    sent("sums", sum_out)
    assert slots.used <= recv_sem.shape[0] and len(outgoing) <= send_sem.shape[0]


def on_chip(sp_size, residual, queries, key_proj, value_proj, diff_lambda, head_gain, out_weight,
            norm_gain, up_weight, down_weight):
    rows, wide = residual.shape
    kw = key_proj.shape[1] // KV_HEADS
    chunk = up_weight.shape[1] // Z_CHIPS
    span = CHIP_CORES * down_weight.shape[1]
    units = Z_CHIPS * Y_CHIPS
    hbm = pl.BlockSpec(memory_space=pltpu.HBM)
    vmem = pl.BlockSpec(memory_space=pltpu.VMEM)
    smem = pl.BlockSpec(memory_space=pltpu.SMEM)
    receives, groups = 68, 12
    return pl.pallas_call(
        fused_kernel,
        out_shape=jax.ShapeDtypeStruct(residual.shape, BF16),
        in_specs=[hbm, hbm, hbm, hbm, smem, vmem, hbm, vmem, hbm, hbm],
        out_specs=vmem,
        scratch_shapes=[
            pltpu.VMEM((sp_size, 2 * key_proj.shape[0], 2 * kw), BF16),
            pltpu.VMEM((sp_size, up_weight.shape[0], chunk), BF16),
            pltpu.VMEM((chunk, sp_size * down_weight.shape[1]), BF16),
            pltpu.VMEM(queries.shape, BF16),
            pltpu.VMEM(residual.shape, BF16),
            pltpu.VMEM(out_weight.shape, BF16),
            pltpu.VMEM((2, rows, wide), BF16),
            pltpu.VMEM((Z_CHIPS, 2, 8, rows), F32),
            pltpu.VMEM((Z_CHIPS, 2, rows, wide), BF16),
            pltpu.VMEM((Z_CHIPS, rows, chunk), BF16),
            pltpu.VMEM((units, Z_CHIPS, rows, span), BF16),
            pltpu.VMEM((units // 2, Z_CHIPS, rows, span), BF16),
            pltpu.VMEM((3, units // 2, rows, span), BF16),
            pltpu.VMEM((4, units // 2, rows, span), BF16),
            pltpu.VMEM((rows, wide), F32),
            pltpu.SemaphoreType.DMA((7,)),
            pltpu.SemaphoreType.DMA((groups,)),
            pltpu.SemaphoreType.DMA((receives,)),
            pltpu.SemaphoreType.REGULAR,
        ],
        compiler_params=pltpu.CompilerParams(
            collective_id=0, has_side_effects=True, vmem_limit_bytes=60 * 2**20
        ),
        name="fused_layer",
    )(residual, queries, key_proj, value_proj, diff_lambda, head_gain.reshape(1, -1), out_weight,
      norm_gain.reshape(1, -1), up_weight, down_weight)


def solution(mesh):
    sp_size, tp_size = mesh.shape["sp"], mesh.shape["tp"]
    direct = tp_size == KV_HEADS == 2 and sp_size == Z_CHIPS * Y_CHIPS * CHIP_CORES
    body = functools.partial(on_chip, sp_size) if direct else on_device
    return jax.shard_map(
        body,
        mesh=mesh,
        in_specs=(
            P("sp", "tp"),
            P("sp", "tp"),
            P(("sp", "tp"), None),
            P(("sp", "tp"), None),
            P(),
            P(),
            P(None, "tp"),
            P("tp"),
            P("sp", "tp"),
            P("tp", "sp"),
        ),
        out_specs=P("sp", "tp"),
        check_vma=False,
    )
```

```python
import functools
import math

import jax
import jax.numpy as jnp
from jax import lax
from jax.experimental import pallas as pl
from jax.experimental.pallas import tpu as pltpu
from jax.sharding import PartitionSpec as P

D = 2048
HEADS = 8
KV_HEADS = 2
HEAD_DIM = 128
VALUE_DIM = 256


epsilon = 1e-06


def head_norm(per_map, lambdas, gain):
    difference = per_map[:, 0] - lambdas[:, None, None] * per_map[:, 1]
    scaled = (
        difference
        * lax.rsqrt(jnp.mean(difference * difference, axis=-1, keepdims=True) + epsilon)
        * gain
    )
    return scaled.astype(jnp.bfloat16)


def on_device(
    residual,
    queries,
    key_proj,
    value_proj,
    diff_lambda,
    head_gain,
    out_weight,
    norm_gain,
    up_weight,
    down_weight,
):
    rows_here = residual.shape[0]
    per_group = HEADS // KV_HEADS
    scaling = HEAD_DIM ** (-0.5)
    all_queries = lax.all_gather(queries, "tp", axis=1, tiled=True)
    query_grid = all_queries.reshape(rows_here, KV_HEADS, per_group, 2, HEAD_DIM)
    stat_shape = (KV_HEADS, per_group, 2, rows_here)
    maxima = jnp.full(stat_shape, -1e30, jnp.float32)
    key_piece = lax.all_gather(key_proj, "sp", axis=0, tiled=True)
    value_piece = lax.all_gather(value_proj, "sp", axis=0, tiled=True)
    key_count = key_piece.shape[0]
    key_grid = key_piece.reshape(key_count, KV_HEADS, 2, HEAD_DIM)
    value_grid = value_piece.reshape(key_count, KV_HEADS, VALUE_DIM)
    scores = (
        jnp.einsum("qagcd,kacd->agcqk", query_grid, key_grid, preferred_element_type=jnp.float32)
        * scaling
    )
    highest = jnp.maximum(maxima, jnp.max(scores, axis=-1))
    weights = jnp.exp(scores - highest[..., None])
    totals = jnp.sum(weights, axis=-1)
    weighted = jnp.einsum(
        "agcqk,kae->agcqe",
        weights.astype(jnp.bfloat16),
        value_grid,
        preferred_element_type=jnp.float32,
    )
    maxima, totals, weighted = (highest, totals, weighted)
    maxima = maxima.reshape(HEADS, 2, rows_here)
    totals = totals.reshape(HEADS, 2, rows_here)
    weighted = weighted.reshape(HEADS, 2, rows_here, VALUE_DIM)
    tp_size = lax.axis_size("tp")
    local_heads = HEADS // tp_size
    got_max, got_tot, got_sum = (
        lax.all_to_all(maxima, "tp", split_axis=0, concat_axis=0, tiled=True),
        lax.all_to_all(totals, "tp", split_axis=0, concat_axis=0, tiled=True),
        lax.all_to_all(weighted, "tp", split_axis=0, concat_axis=0, tiled=True),
    )
    got_max = got_max.reshape(tp_size, local_heads, 2, rows_here)
    got_tot = got_tot.reshape(tp_size, local_heads, 2, rows_here)
    got_sum = got_sum.reshape(tp_size, local_heads, 2, rows_here, VALUE_DIM)
    highest = jnp.max(got_max, axis=0)
    factor = jnp.exp(got_max - highest)
    totals_all = jnp.sum(factor * got_tot, axis=0)
    sums_all = jnp.sum(factor[..., None] * got_sum, axis=0)
    lambdas = lax.dynamic_slice_in_dim(diff_lambda, lax.axis_index("tp") * local_heads, local_heads)
    own_heads = head_norm(sums_all / totals_all[..., None], lambdas, head_gain)
    head_outputs = lax.all_gather(own_heads, "tp", axis=0, tiled=True)
    out_grid = out_weight.reshape(HEADS, VALUE_DIM, out_weight.shape[1])
    projected = jnp.einsum(
        "hqe,hed->qd", head_outputs, out_grid, preferred_element_type=jnp.float32
    )
    after_mix = residual.astype(jnp.float32) + projected
    squares = lax.psum(jnp.sum(after_mix * after_mix, axis=1), "tp")
    normed = (after_mix * lax.rsqrt(squares / D + epsilon)[:, None] * norm_gain).astype(
        jnp.bfloat16
    )
    full_rows = lax.all_gather(normed, "tp", axis=1, tiled=True)
    hidden = jnp.dot(
        full_rows,
        lax.all_gather(up_weight, "sp", axis=0, tiled=True),
        preferred_element_type=jnp.float32,
    )
    activated = jnp.square(jax.nn.relu(hidden)).astype(jnp.bfloat16)
    partial_value = jnp.dot(
        activated,
        lax.all_gather(down_weight, "sp", axis=1, tiled=True),
        preferred_element_type=jnp.float32,
    )
    mixer_sum = lax.psum_scatter(partial_value, "tp", scatter_dimension=1, tiled=True)
    return (after_mix + mixer_sum).astype(jnp.bfloat16)


MESH = pl.DeviceIdType.MESH
F32 = jnp.float32
BF16 = jnp.bfloat16
CHIP_CORES = 2
Y_CHIPS = 2
Z_CHIPS = 4
OWN, NEAR, FAR, MID = range(Z_CHIPS)


class Slots:
    def __init__(self):
        self.used = 0

    def take(self, count):
        base = self.used
        self.used += count
        return base


def fused_kernel(
    residual, queries, keys, values, lambdas, head_gain, out_weight, norm_gain,
    up, down, out,
    kv_all, up_all, down_all, q_buf, res_buf, w_buf, heads_all, squares, tokens, act,
    parts, parts_in, sum_out, sum_in, after, local_sem, send_sem, recv_sem, go,
):
    x = lax.axis_index("tp")
    s = lax.axis_index("sp")
    core, y, z = s % CHIP_CORES, (s // CHIP_CORES) % Y_CHIPS, s // (CHIP_CORES * Y_CHIPS)

    def place(z_, y_, c_):
        return (z_ * Y_CHIPS + y_) * CHIP_CORES + c_

    half = z // 2
    inner = ((z + 1) // 2) % 2
    z_near = 4 * half + 1 - z
    z_in, z_out = 2 - half, 3 - 3 * half
    is_inner, is_outer = inner == 1, inner == 0
    same = 1 - (x + half) % 2
    sends_far, keeps_far = same == 1, same == 0

    def in_column(z_):
        return {"sp": place(z_, y, core), "tp": x}

    mate = {"sp": s, "tp": 1 - x}
    beside = {"sp": place(z, 1 - y, core), "tp": x}
    twin = {"sp": place(z, y, 1 - core), "tp": x}
    near, across, beyond = in_column(z_near), in_column(z_in), in_column(z_out)

    barrier = pltpu.get_barrier_semaphore()
    peers = [mate, beside, twin, near, across, beyond]
    for peer in peers:
        pl.semaphore_signal(barrier, inc=1, device_id=peer, device_id_type=MESH)

    local_copies = []
    slots = Slots()
    outgoing = {}

    def bring(src, dst):
        copy = pltpu.make_async_copy(src, dst, local_sem.at[len(local_copies)])
        local_copies.append(copy)
        copy.start()
        return copy

    def send(src, dst, peer, slot, group, when=None):
        i = outgoing.setdefault(group, len(outgoing))

        def start():
            pltpu.make_async_remote_copy(
                src_ref=src, dst_ref=dst, send_sem=send_sem.at[i], recv_sem=recv_sem.at[slot],
                device_id=peer, device_id_type=MESH,
            ).start()

        if when is None:
            start()
        else:
            pl.when(when)(start)

    def sent(group, whole, when=None):
        def wait():
            pltpu.make_async_remote_copy(
                src_ref=whole, dst_ref=whole, send_sem=send_sem.at[outgoing[group]],
                recv_sem=recv_sem.at[0], device_id=mate, device_id_type=MESH,
            ).wait_send()

        if when is None:
            wait()
        else:
            pl.when(when)(wait)

    def arrive(dst, slot, when=None):
        if when is not None:
            pl.when(when)(lambda: arrive(dst, slot))
            return
        pltpu.make_async_remote_copy(
            src_ref=dst, dst_ref=dst, send_sem=send_sem.at[0], recv_sem=recv_sem.at[slot],
            device_id=mate, device_id_type=MESH,
        ).wait_recv()

    few = keys.shape[0]
    kw = kv_all.shape[2] // 2
    chunk = up_all.shape[2]
    lanes = down.shape[1]

    def half_of(ref, part):
        return ref.at[:, pl.ds(pl.multiple_of(part * kw, kw), kw)]

    def kv_rows(block, part, side):
        return kv_all.at[block, pl.ds(pl.multiple_of(part * few, few), few), pl.ds(side * kw, kw)]

    own_kv = [bring(half_of(keys, x), kv_rows(s, x, 0)), bring(half_of(values, x), kv_rows(s, x, 1))]
    q_copy = bring(queries, q_buf)

    pl.semaphore_wait(barrier, len(peers))

    swap = slots.take(1)
    for side, ref in enumerate((keys, values)):
        send(half_of(ref, 1 - x), kv_rows(s, x, side), mate, swap, "swap")
    w_copy = bring(out_weight, w_buf)
    r_copy = bring(residual, res_buf)

    def up_chunk(part):
        return up.at[:, pl.ds(pl.multiple_of(part * chunk, chunk), chunk)]

    def down_chunk(part):
        return down.at[pl.ds(pl.multiple_of(part * chunk, chunk), chunk), :]

    def kv_block(b):
        return kv_all.at[b]

    def up_block(b):
        return up_all.at[b]

    def down_block(b):
        return down_all.at[:, pl.ds(pl.multiple_of(b * lanes, lanes), lanes)]

    up_own = bring(up_chunk(z), up_block(s))
    down_own = bring(down_chunk(z), down_block(s))

    def relay(block, base, j):
        z_ = (z_in, z_out)[j]
        send(block(z_), block(z_), near, base + 1 + j, "kv_relay", is_inner)

    class Stream:
        def __init__(self, name, block_of, order, staged=False):
            self.name, self.block_of, self.order = name, block_of, order
            self.z, self.y = slots.take(Z_CHIPS), slots.take(Z_CHIPS)
            self.step = int(staged)
            self.twin = slots.take(2 * Z_CHIPS if staged else 1)
            self.far = self.twin + Z_CHIPS * self.step

        def block(self, k, y_, c_):
            return self.block_of(place(self.order[k], y_, c_))

        def spread(self, k, when=None):
            b = self.block(k, y, core)
            if k != OWN:
                arrive(b, self.z + k, when)
            send(b, b, beside, self.y + k, self.name, when)
            send(b, b, twin, self.twin + k * self.step, self.name, when)

        def pass_on(self, k):
            b = self.block(k, 1 - y, core)
            arrive(b, self.y + k)
            send(b, b, twin, self.far + k * self.step, self.name)

        def wait_twin(self, k, side=None):
            if side != 1:
                arrive(self.block(k, y, 1 - core), self.twin + k)
            if side != 0:
                arrive(self.block(k, 1 - y, 1 - core), self.far + k)

    kv = Stream("kv", kv_block, (z, z_near, z_in, z_out))
    ups = Stream("up", up_block, (z, z_near, z_out, z_in))
    downs = Stream("down", down_block, (
        z,
        same * z_out + (1 - same) * z_near,
        same * z_in + (1 - same) * z_out,
        same * z_near + (1 - same) * z_in,
    ), staged=True)

    def deal(stream, piece_of, k, when=None):
        z_, peer, slot = {
            NEAR: (z_near, near, NEAR), FAR: (z_out, beyond, FAR + inner), MID: (z_in, across, FAR + inner),
        }[k]
        if stream is downs:
            theirs = same if k == NEAR else 1 - same
            slot = 1 + (slot - 1 + 2 * theirs) % 3
        send(piece_of(z_), stream.block_of(s), peer, stream.z + slot, stream.name, when)

    def kv_onward(k):
        b = kv.block(k, y, core)
        send(b, b, beside, kv.y + k, "kv")
        send(b, b, twin, kv.twin, "kv")

    def column_kv(z_):
        return kv_block(place(z_, y, core))

    outlets = (
        (beside, kv.y), (twin, kv.twin), (near, kv.z + 1), (across, kv.z + 3 - inner)
    )
    for peer, slot in outlets:
        for side, ref in enumerate((keys, values)):
            send(half_of(ref, x), kv_rows(s, x, side), peer, slot, "kv")
    mates_rows = kv_all.at[s, pl.ds(pl.multiple_of((1 - x) * few, few), few), :]
    arrive(mates_rows, swap)
    for peer, slot in outlets:
        send(mates_rows, mates_rows, peer, slot, "kv")
    deal(ups, up_chunk, NEAR, is_outer)
    deal(ups, up_chunk, MID)
    kv.spread(1)
    arrive(kv.block(2, y, core), kv.z + 2)
    relay(column_kv, kv.z + 1, 0)
    arrive(kv.block(3, y, core), kv.z + 3, is_inner)
    relay(column_kv, kv.z + 1, 1)
    deal(ups, up_chunk, NEAR, is_inner)
    kv_onward(2)
    arrive(kv.block(3, y, core), kv.z + 3, is_outer)
    deal(ups, up_chunk, FAR)
    kv_onward(3)
    up_own.wait()
    ups.spread(OWN)
    for copy in own_kv:
        copy.wait()
    for k in range(Z_CHIPS):
        kv.pass_on(k)
    arrive(kv_all.at[pl.ds(0, 2 * Z_CHIPS)], kv.twin)
    q_copy.wait()

    local_heads = q_buf.shape[1] // (2 * HEAD_DIM)
    blocks, per_block = kv_all.shape[0], kv_all.shape[1]
    key_count = blocks * per_block
    factor = HEAD_DIM ** (-0.5) * math.log2(math.e)
    vals = lambda: kv_all[:, :, kw:].reshape(key_count, kw)
    heads = slots.take(1)

    def head_cols(part, h):
        return heads_all.at[part, :, pl.ds(h * VALUE_DIM, VALUE_DIM)]

    for h in range(local_heads):
        maps = []
        for c in range(2):
            q = q_buf[:, (2 * h + c) * HEAD_DIM : (2 * h + c + 1) * HEAD_DIM]
            k = kv_all[:, :, c * HEAD_DIM : (c + 1) * HEAD_DIM].reshape(key_count, HEAD_DIM)
            scores = lax.dot_general(q, k, (((1,), (1,)), ((), ())), preferred_element_type=F32)
            top = jnp.max(scores, axis=1, keepdims=True)
            weights = jnp.exp2((scores - top) * factor)
            total = jnp.sum(weights, axis=1, keepdims=True)
            summed = jnp.dot(weights.astype(BF16), vals(), preferred_element_type=F32)
            maps.append(summed / total)
        diff = maps[0] - lambdas[x * local_heads + h] * maps[1]
        scaled = diff * lax.rsqrt(jnp.mean(diff * diff, axis=1, keepdims=True) + epsilon)
        heads_all[x, :, pl.ds(h * VALUE_DIM, VALUE_DIM)] = (scaled * head_gain[...]).astype(BF16)
        send(head_cols(x, h), head_cols(x, h), mate, heads, "heads")
        if h < 2:
            ups.spread((NEAR, FAR)[h], is_inner)
    ups.spread(MID, is_inner)
    ups.spread(NEAR, is_outer)
    ups.pass_on(OWN)

    wide = heads_all.shape[2]
    rows = heads_all.shape[1]
    w_copy.wait()
    r_copy.wait()

    def w_rows(part):
        return w_buf[pl.ds(pl.multiple_of(part * wide, wide), wide), :]

    mix = res_buf[...].astype(F32) + jnp.dot(heads_all[x], w_rows(x), preferred_element_type=F32)
    arrive(heads_all.at[1 - x], heads)
    mix = mix + jnp.dot(heads_all[1 - x], w_rows(1 - x), preferred_element_type=F32)
    after[...] = mix
    own_squares = jnp.sum(mix * mix, axis=1, keepdims=True)
    width = 2 * wide
    tokens[z, x] = (mix * norm_gain[...]).astype(BF16)
    squares[z, x] = jnp.broadcast_to(own_squares, (rows, rows)).T[: squares.shape[2]]

    token_z = slots.take(2 * (Z_CHIPS - 1))
    token_x = slots.take(2 * Z_CHIPS)

    def send_tokens(z_, peer, slot, when=None, group="token"):
        for n, ref in enumerate((tokens, squares)):
            send(ref.at[z_, x], ref.at[z_, x], peer, slot + n, (group, n), when)

    def take_tokens(z_, part, slot, when=None):
        for n, ref in enumerate((tokens, squares)):
            arrive(ref.at[z_, part], slot + n, when)

    def collect(j, when):
        z_ = (z_in, z_out)[j]
        take_tokens(z_, x, token_z + 2 + 2 * j, when)
        if when is is_inner:
            send_tokens(z_, near, token_z + 2 + 2 * j, when, "relay")
        send_tokens(z_, mate, token_x + 4 + 2 * j, when)

    send_tokens(z, near, token_z)
    send_tokens(z, across, token_z + 4 - 2 * inner)
    send_tokens(z, mate, token_x)
    deal(downs, down_chunk, NEAR, keeps_far)
    deal(downs, down_chunk, MID)
    deal(downs, down_chunk, NEAR, is_outer & sends_far)
    ups.spread(FAR, is_outer)
    ups.spread(MID, is_outer)
    down_own.wait()
    downs.spread(OWN)
    take_tokens(z_near, x, token_z)
    send_tokens(z_near, mate, token_x + 2)
    collect(0, is_inner)
    collect(1, is_inner)
    deal(downs, down_chunk, NEAR, is_inner & sends_far)
    for k in (NEAR, FAR, MID):
        ups.pass_on(k)
    collect(0, is_outer)
    arrive(up_all.at[pl.ds(0, 2 * Z_CHIPS)], ups.twin)

    halves = up_all.shape[0] // 2

    def up_rows(i):
        return up_all[i * halves : (i + 1) * halves].reshape(wide, chunk)

    def activate(pair):
        first = pl.ds(2 * pair, 2)
        hidden = jnp.dot(
            tokens[first, 0].reshape(2 * rows, wide), up_rows(0), preferred_element_type=F32
        ) + jnp.dot(
            tokens[first, 1].reshape(2 * rows, wide), up_rows(1), preferred_element_type=F32
        )
        factors = []
        for i in range(2):
            mean = (squares[2 * pair + i, 0] + squares[2 * pair + i, 1])[:1] / width
            factors.append(jnp.broadcast_to(lax.rsqrt(mean + epsilon), (rows, rows)).T[:, :1])
        hidden = hidden * jnp.concatenate(factors, axis=0)
        act[first] = jnp.square(jnp.maximum(hidden, 0.0)).astype(BF16).reshape(2, rows, chunk)

    span = parts.shape[3]
    part_slot = slots.take(2 * Z_CHIPS)
    pairs = (pl.ds(2 * half, 2), pl.ds(2 * (1 - half), 2))
    sides = (y, 1 - y)

    def project(k, side, i, when=None):
        unit = Y_CHIPS * downs.order[k] + sides[side]
        cols = down_all[:, pl.ds(pl.multiple_of(unit * span, span), span)]
        product = jnp.dot(
            act[pairs[i]].reshape(2 * rows, chunk), cols, preferred_element_type=F32
        )
        parts[unit, pairs[i]] = product.astype(BF16).reshape(2, rows, span)
        if when is not False:
            kept = unit % Z_CHIPS
            send(parts.at[unit, pairs[i]], parts_in.at[kept, pairs[i]], mate,
                 part_slot + 2 * kept + i, "parts", when)

    for i, z_ in enumerate((z, z_near)):
        take_tokens(z_, 1 - x, token_x + 2 * i)
    activate(half)
    sent(("relay", 0), tokens.at[0], is_inner)
    sent(("relay", 1), squares.at[0], is_inner)

    @pl.when(is_inner)
    def _():
        for peer in (across, beyond):
            pl.semaphore_signal(go, inc=1, device_id=peer, device_id_type=MESH)
        pl.semaphore_wait(go, 1)

    deal(downs, down_chunk, FAR, is_inner)
    downs.wait_twin(OWN, 0)
    project(OWN, 0, 0, keeps_far)
    downs.spread(1, is_inner | keeps_far)

    @pl.when(is_outer)
    def _():
        pl.semaphore_wait(go, 1)

    deal(downs, down_chunk, FAR, is_outer)
    collect(1, is_outer)
    downs.pass_on(OWN)
    downs.wait_twin(OWN, 1)
    project(OWN, 1, 0, keeps_far)
    downs.spread(2, is_inner)
    downs.spread(3, is_inner)
    downs.spread(1, is_outer & sends_far)
    downs.wait_twin(1, 0)
    project(1, 0, 0)
    for i, z_ in ((2, z_in), (3, z_out)):
        take_tokens(z_, 1 - x, token_x + 2 * i)
    activate(1 - half)
    for side in range(2):
        project(OWN, side, 1, keeps_far)
    project(1, 0, 1)
    downs.spread(2, is_outer)
    downs.pass_on(1)
    downs.wait_twin(1, 1)
    for i in (1, 0):
        project(1, 1, i)
    downs.wait_twin(2, 0)
    for i in (1, 0):
        project(2, 0, i, sends_far)
    downs.spread(3, is_outer)
    downs.pass_on(2)
    downs.wait_twin(2, 1)
    for i in (1, 0):
        project(2, 1, i, sends_far)

    sum_slot, pass_slot = slots.take(2), slots.take(2 * Z_CHIPS)

    def deliver(i, u, row, peer, when):
        slot = sum_slot + row if row < 2 else pass_slot + Z_CHIPS * (row - 2) + u
        send(sum_out.at[i, u], sum_in.at[row, u], peer, slot, "sums", when)

    def both(u, z_):
        return parts[Z_CHIPS * x + u, z_].astype(F32) + parts_in[u, z_].astype(F32)

    def settle_far(u, when):
        arrive(parts_in.at[u, pairs[1]], part_slot + 2 * u + 1, when)
        for j, z_ in enumerate((z_in, z_out)):

            @pl.when(when & is_outer)
            def _():
                sum_out[1 + j, u] = both(u, z_).astype(BF16)

            deliver(1 + j, u, 2 + j, near, when & is_outer)

            @pl.when(when & is_inner)
            def _():
                mine = both(u, z_)
                arrive(sum_in.at[2 + j, u], pass_slot + Z_CHIPS * j + u)
                sum_out[1 + j, u] = (mine + sum_in[2 + j, u].astype(F32)).astype(BF16)

            deliver(1 + j, u, 1, (across, beyond)[j], when & is_inner)

    def settle_half(u, when):
        arrive(parts_in.at[u, pairs[0]], part_slot + 2 * u, when)

        @pl.when(when)
        def _():
            sum_out[0, u] = both(u, z_near).astype(BF16)

        deliver(0, u, 0, near, when)

        @pl.when(when)
        def _():
            cols = pl.ds(pl.multiple_of(u * span, span), span)
            after[:, cols] = after[:, cols] + both(u, z)

    def columns(a):
        return [Y_CHIPS * a + side for side in sides]

    outer_sends, inner_sends = sends_far & is_outer, sends_far & is_inner
    for u in columns(half):
        settle_far(u, outer_sends)
    downs.wait_twin(3, 0)
    for i in (1, 0):
        project(3, 0, i, False)
    downs.pass_on(3)
    downs.wait_twin(3, 1)
    for i in (1, 0):
        project(3, 1, i, False)
    for u in columns(1 - half):
        settle_far(u, outer_sends)
        settle_half(u, inner_sends)
    for u in columns(half):
        settle_half(u, outer_sends)
        settle_far(u, inner_sends)
        settle_half(u, inner_sends)
    for u in columns(1 - half):
        settle_half(u, outer_sends)
        settle_far(u, inner_sends)
    for u in columns(z_out % 2) + columns(z_in % 2):
        settle_far(u, keeps_far & is_outer)
        settle_half(u, keeps_far)
        settle_far(u, keeps_far & is_inner)

    for group, whole in (
        ("swap", kv_all.at[0, pl.ds(0, few), :]),
        ("kv", kv_all.at[pl.ds(0, 3 * Z_CHIPS + 2)]),
        ("up", up_all.at[pl.ds(0, 4 * Z_CHIPS - 1)]),
        ("down", down_all.at[:, pl.ds(0, (4 * Z_CHIPS - 1) * lanes)]),
        ("heads", heads_all.at[0]),
        (("token", 0), tokens.at[pl.ds(0, 3)]),
        (("token", 1), squares.at[pl.ds(0, 3)]),
        ("parts", parts.at[pl.ds(0, Z_CHIPS)]),
    ):
        sent(group, whole)
    sent("kv_relay", kv_all.at[pl.ds(0, 2)], is_inner)
    for row in range(2):
        arrive(sum_in.at[row], sum_slot + row)
    for u in range(Z_CHIPS):
        cols = slice(u * span, (u + 1) * span)
        total = after[:, cols] + sum_in[0, u].astype(F32) + sum_in[1, u].astype(F32)
        out[:, cols] = total.astype(out.dtype)
    sent("sums", sum_out)
    assert slots.used <= recv_sem.shape[0] and len(outgoing) <= send_sem.shape[0]


def on_chip(sp_size, residual, queries, key_proj, value_proj, diff_lambda, head_gain, out_weight,
            norm_gain, up_weight, down_weight):
    rows, wide = residual.shape
    kw = key_proj.shape[1] // KV_HEADS
    chunk = up_weight.shape[1] // Z_CHIPS
    span = CHIP_CORES * down_weight.shape[1]
    units = Z_CHIPS * Y_CHIPS
    hbm = pl.BlockSpec(memory_space=pltpu.HBM)
    vmem = pl.BlockSpec(memory_space=pltpu.VMEM)
    smem = pl.BlockSpec(memory_space=pltpu.SMEM)
    receives, groups = 68, 12
    return pl.pallas_call(
        fused_kernel,
        out_shape=jax.ShapeDtypeStruct(residual.shape, BF16),
        in_specs=[hbm, hbm, hbm, hbm, smem, vmem, hbm, vmem, hbm, hbm],
        out_specs=vmem,
        scratch_shapes=[
            pltpu.VMEM((sp_size, 2 * key_proj.shape[0], 2 * kw), BF16),
            pltpu.VMEM((sp_size, up_weight.shape[0], chunk), BF16),
            pltpu.VMEM((chunk, sp_size * down_weight.shape[1]), BF16),
            pltpu.VMEM(queries.shape, BF16),
            pltpu.VMEM(residual.shape, BF16),
            pltpu.VMEM(out_weight.shape, BF16),
            pltpu.VMEM((2, rows, wide), BF16),
            pltpu.VMEM((Z_CHIPS, 2, 8, rows), F32),
            pltpu.VMEM((Z_CHIPS, 2, rows, wide), BF16),
            pltpu.VMEM((Z_CHIPS, rows, chunk), BF16),
            pltpu.VMEM((units, Z_CHIPS, rows, span), BF16),
            pltpu.VMEM((units // 2, Z_CHIPS, rows, span), BF16),
            pltpu.VMEM((3, units // 2, rows, span), BF16),
            pltpu.VMEM((4, units // 2, rows, span), BF16),
            pltpu.VMEM((rows, wide), F32),
            pltpu.SemaphoreType.DMA((7,)),
            pltpu.SemaphoreType.DMA((groups,)),
            pltpu.SemaphoreType.DMA((receives,)),
            pltpu.SemaphoreType.REGULAR,
        ],
        compiler_params=pltpu.CompilerParams(
            collective_id=0, has_side_effects=True, vmem_limit_bytes=60 * 2**20
        ),
        name="fused_layer",
    )(residual, queries, key_proj, value_proj, diff_lambda, head_gain.reshape(1, -1), out_weight,
      norm_gain.reshape(1, -1), up_weight, down_weight)


def solution(mesh):
    sp_size, tp_size = mesh.shape["sp"], mesh.shape["tp"]
    direct = tp_size == KV_HEADS == 2 and sp_size == Z_CHIPS * Y_CHIPS * CHIP_CORES
    body = functools.partial(on_chip, sp_size) if direct else on_device
    return jax.shard_map(
        body,
        mesh=mesh,
        in_specs=(
            P("sp", "tp"),
            P("sp", "tp"),
            P(("sp", "tp"), None),
            P(("sp", "tp"), None),
            P(),
            P(),
            P(None, "tp"),
            P("tp"),
            P("sp", "tp"),
            P("tp", "sp"),
        ),
        out_specs=P("sp", "tp"),
        check_vma=False,
    )
```
